32 devices in a mesh: fs: 8 (over z, y), tp: 4 (over x, core).
Axes of the slice: x: 2, y: 2, z: 4, core: 2. Of those that a mesh axis runs over, the one named last changes fastest.
Arguments:
- prompt: bfloat16 [6144, 2048], P('fs'), may hold values from -6 to 6
- routes: int32 [6144, 2], P('fs'), may hold values from 0 to 15, all different within a row; in each aligned block of 768 rows (0 to 767, 768 to 1535, ...) at most 192 rows name the same one
- affinity: float32 [6144, 2], P('fs'), may hold values from 0.05 to 1
- norm_gain: float32 [2048], P('fs'), may hold values from 0.1 to 1.9
- gate_master: float32 [16, 2048, 1024], P(None, 'fs', 'tp'), may hold values from -0.125 to 0.125
- up_master: float32 [16, 2048, 1024], P(None, 'fs', 'tp'), may hold values from -0.125 to 0.125
- down_master: float32 [16, 1024, 2048], P(None, 'fs', 'tp'), may hold values from -0.1875 to 0.1875
Outputs:
- mixed: bfloat16 [6144, 2048], P('fs', 'tp')
- gate_weights: bfloat16 [16, 2048, 1024], P('fs', None, 'tp')
- up_weights: bfloat16 [16, 2048, 1024], P('fs', None, 'tp')
- down_weights: bfloat16 [16, 1024, 2048], P('fs', None, 'tp')
The draws below stay inside these ranges and needn't reach their ends.
Inputs may be any that keep to these rules, and one draw needn't show every extreme that they name: `routes`: each row names 2 different experts. In each aligned block of 768 rows no expert is named more than 192 times, a bound that some block reaches.
All inputs are finite; a program needn't handle non-finite values.
Results may differ from the reference program's by a relative error of at most 0.0086.
Values may be sent and summed in bfloat16 or wider, within the bound.
A program may use at most 128 MiB of HBM per device.

```python
import math
import jax
import jax.numpy as jnp
import numpy as np
from jax import lax

D = 2048
FF = 1024
TOP = 2
TOK_DEV = 768
EXPERTS = 16
TOKENS = 6144
CAP = 192
N_FS = 8


def block_levels(key, extent, split, smallest, top_value):
    def one(position, parts):
        draws = jax.random.uniform(jax.random.fold_in(jax.random.fold_in(key, 6), position), (parts,), jnp.float32, smallest / len(split), top_value / len(split))
        return jnp.repeat(jnp.exp(draws), extent[position] // parts).reshape((-1,) + (1,) * (len(extent) - position - 1))

    level = one(*split[0])
    for cut in split[1:]:
        level = level * one(*cut)
    return level


def assign_block(key, own, number, rows, amount, top, most, slope):
    ranking = jax.random.permutation(key, amount)
    crowded, common = shares(amount, rows * top, most, slope, True), shares(amount, rows * top, most, slope, False)
    places = jnp.arange(amount)

    def named(lengths, turn):
        used = int((lengths > 0).sum())
        fixed = max(1, used // 4)
        moved = fixed + (places - fixed + turn * (used - fixed)) % max(1, amount - fixed)
        return jnp.zeros((amount,), jnp.int32).at[ranking[jnp.where(places < fixed, places, moved)]].set(jnp.asarray(lengths, jnp.int32))

    lengths = jnp.where(number % 4 == 0, named(crowded, number // 4), named(common, number - number // 4 - 1))
    mixed = jax.random.permutation(jax.random.fold_in(own, 3), amount)
    source_of, taker = mixed[0:amount // 2 * 2:2], mixed[1:amount // 2 * 2:2]
    margin = jnp.minimum(lengths[source_of] - 1, most - lengths[taker]) // 2
    margin = jnp.where((source_of == ranking[0]) | (taker == ranking[0]) | (lengths[taker] == 0), 0, jnp.maximum(margin, 0))
    moved = jax.random.randint(jax.random.fold_in(own, 4), (amount // 2,), 0, 1 << 20) % (margin + 1)
    lengths = lengths.at[source_of].add(-moved).at[taker].add(moved)
    labels = jnp.searchsorted(jnp.cumsum(lengths), jnp.arange(rows * top), side="right").astype(jnp.int32)
    grid = labels.reshape(top, rows).T
    grid = grid[jax.random.permutation(jax.random.fold_in(own, 1), rows)]
    turn = jax.random.randint(jax.random.fold_in(own, 2), (rows, 1), 0, top)
    return jnp.take_along_axis(grid, (jnp.arange(top)[None, :] + turn) % top, axis=1)


def shares(count, total, bound, slope, full):
    weights = [(1 << 20) // math.isqrt(rank ** slope) + 1 for rank in range(1, count + 1)]
    largest = bound if full else min(bound, max(-(-total // count), total * weights[0] // sum(weights)))
    least = 1 if total - largest >= count - 1 else 0
    counts, rest = [largest] + [least] * (count - 1), total - largest - least * (count - 1)
    while rest > 0:
        free = [i for i in range(1, count) if counts[i] < largest] or [i for i in range(1, count) if counts[i] < bound]
        whole, left = sum([weights[i] for i in free]), rest
        for i in free:
            extra = min(bound - counts[i], max(1, left * weights[i] // whole), rest)
            counts[i] = counts[i] + extra
            rest = rest - extra
    return np.array(counts)


def noise(rng, dims, width, most, pieces=(), kind=jnp.bfloat16):
    gain = block_levels(rng, dims, pieces, -0.22, 0.18) if pieces else 1.0
    drawn = jax.random.normal(rng, dims, jnp.float32) * width * gain
    return jnp.minimum(jnp.maximum(drawn, -most), most).astype(kind)


def setup_inputs(seed: int = 0) -> dict:
    arg_keys = jax.random.split(jax.random.key(seed), 8)
    prompt = noise(arg_keys[0], (TOKENS, D), 1.0, 6.0, ((0, 8),))
    routes_keys = jax.random.split(jax.random.fold_in(arg_keys[1], 1), TOKENS // TOK_DEV)
    routes_turns = jax.random.permutation(jax.random.fold_in(arg_keys[1], 3), TOKENS // TOK_DEV)
    routes = jax.vmap(lambda own, number: assign_block(jax.random.fold_in(arg_keys[1], 2), own, number, TOK_DEV, EXPERTS, TOP, CAP, 2))(routes_keys, routes_turns).reshape((TOKENS, TOP))
    affinity = jnp.clip(0.05 + 0.95 * jax.random.uniform(arg_keys[2], (TOKENS, TOP), jnp.float32) ** block_levels(arg_keys[2], (TOKENS, TOP), ((0, 8),), -0.2, 0.2), 0.05, 1.0)
    norm_gain = jnp.clip(1.0 + 0.18 * jax.random.normal(arg_keys[3], (D,), jnp.float32), 0.1, 1.9)
    gate_master = noise(arg_keys[4], (EXPERTS, D, FF), D ** -0.5, 0.125, ((1, 8), (2, 4)), jnp.float32)
    up_master = noise(arg_keys[5], (EXPERTS, D, FF), D ** -0.5, 0.125, ((1, 8), (2, 4)), jnp.float32)
    down_master = noise(arg_keys[6], (EXPERTS, FF, D), FF ** -0.5, 0.1875, ((1, 8), (2, 4)), jnp.float32)
    return {"prompt": prompt, "routes": routes, "affinity": affinity, "norm_gain": norm_gain, "gate_master": gate_master, "up_master": up_master, "down_master": down_master}


norm_eps = 1e-06

def one_expert(operands):
    slot_rows, gate_weight, up_weight, down_weight = operands
    gate_pre = jnp.dot(slot_rows, gate_weight, preferred_element_type=jnp.float32)
    up_pre = jnp.dot(slot_rows, up_weight, preferred_element_type=jnp.float32)
    hidden = (jax.nn.silu(gate_pre) * up_pre).astype(jnp.bfloat16)
    return jnp.dot(hidden, down_weight, preferred_element_type=jnp.float32).astype(jnp.bfloat16)

def reference(prompt, routes, affinity, norm_gain, gate_master, up_master, down_master):
    gain_rows = norm_gain[None, :, None]
    gate_weights = (gate_master * gain_rows).astype(jnp.bfloat16)
    up_weights = (up_master * gain_rows).astype(jnp.bfloat16)
    down_weights = down_master.astype(jnp.bfloat16)
    values = prompt.astype(jnp.float32)
    normed = (values * lax.rsqrt(lax.optimization_barrier(jnp.mean(values * values, axis=-1, keepdims=True)) + norm_eps)).astype(jnp.bfloat16)
    flat_ids = routes.reshape(N_FS, TOK_DEV * TOP)
    onehot = (flat_ids[:, :, None] == jnp.arange(EXPERTS, dtype=jnp.int32)[None, None, :]).astype(jnp.int32)
    slot_rank = lax.optimization_barrier(jnp.sum(jnp.cumsum(onehot, axis=1) * onehot, axis=2)) - 1
    column = (jnp.arange(N_FS, dtype=jnp.int32)[:, None] * CAP + slot_rank).reshape(-1).astype(jnp.int32)
    expert_of = flat_ids.reshape(-1).astype(jnp.int32)
    token_of = (jnp.arange(TOKENS * TOP, dtype=jnp.int32) // TOP).astype(jnp.int32)
    buffer = jnp.zeros((EXPERTS, N_FS * CAP, D), jnp.bfloat16).at[expert_of, column].set(normed[token_of])
    outputs = lax.map(one_expert, (buffer, gate_weights, up_weights, down_weights))
    picked = outputs[expert_of, column].reshape(TOKENS, TOP, D).astype(jnp.float32)
    share = affinity / lax.optimization_barrier(jnp.sum(affinity, axis=1, keepdims=True))
    mixed = lax.optimization_barrier(jnp.sum(share[:, :, None] * picked, axis=1)).astype(jnp.bfloat16)
    return (mixed, gate_weights, up_weights, down_weights)
```

```python
import functools

import jax
import jax.numpy as jnp
from jax import lax
from jax.experimental import pallas as pl
from jax.experimental.pallas import tpu as pltpu
from jax.sharding import PartitionSpec as P

norm_eps = 1e-06
MESH = pl.DeviceIdType.MESH
RING = 4


def remote(src, dst, send_sem, recv_sem, where):
    return pltpu.make_async_remote_copy(
        src_ref=src,
        dst_ref=dst,
        send_sem=send_sem,
        recv_sem=recv_sem,
        device_id=where,
        device_id_type=MESH,
    )


def loop(first, last, body):
    def step(i, carry):
        body(i)
        return carry

    lax.fori_loop(first, last, step, 0)


def span(index, size):
    return pl.ds(pl.multiple_of(index * size, size), size)


def far_first(z, depth, i):
    low, high = z, depth - 1 - z
    skew = jnp.abs(low - high)
    reach = jnp.minimum(low, high)
    j = i - skew
    distance = reach - j // 2
    paired = jnp.where(j % 2 == 0, z + distance, z - distance)
    single = jnp.where(low > high, i, depth - 1 - i)
    return jnp.where(i < skew, single, paired)


class Spread:
    def __init__(self, tp, whole, rows, width, sems):
        self.chips = tp // 2
        self.me = lax.axis_index("tp")
        self.chip, self.core = self.me // 2, self.me % 2
        self.whole, self.rows, self.width = whole, rows, width
        self.first_send, self.first_recv, self.relay_send, self.relay_recv = sems

    def target(self, hop):
        if hop == 0:
            return self.chip * 2 + 1 - self.core
        return lax.rem(self.chip + hop, self.chips) * 2 + self.core

    def block(self, chunk, owner):
        return self.whole.at[:, span(chunk, self.rows), span(owner, self.width)]

    def first(self, chunk, hop):
        mine = self.block(chunk, self.me)
        return remote(mine, mine, self.first_send.at[chunk, hop], self.first_recv.at[chunk, hop], {"tp": self.target(hop)})

    def relay(self, chunk, hop):
        owner = lax.rem(self.chip - hop + self.chips, self.chips) * 2 + self.core
        taken = self.block(chunk, owner)
        return remote(taken, taken, self.relay_send.at[chunk, hop], self.relay_recv.at[chunk, hop], {"tp": self.target(0)})

    def start(self, chunk):
        for hop in [*range(1, self.chips), 0]:
            self.first(chunk, hop).start()

    def hand_on(self, chunk):
        for hop in range(1, self.chips):
            self.first(chunk, hop).wait_recv()
            self.relay(chunk, hop).start()

    def arrive(self, chunk):
        self.first(chunk, 0).wait_recv()
        for hop in range(1, self.chips):
            self.relay(chunk, hop).wait_recv()

    def drain(self, chunk):
        for hop in range(self.chips):
            self.first(chunk, hop).wait_send()
        for hop in range(1, self.chips):
            self.relay(chunk, hop).wait_send()


def spread_sems(chunks, tp):
    return [pltpu.SemaphoreType.DMA((chunks, tp // 2))] * 4


class Weights:
    def __init__(self, n, master, gain, held, raw, send, load_sem, send_sem, recv_sem):
        self.n, self.master, self.gain, self.held, self.raw, self.send = n, master, gain, held, raw, send
        self.load_sem, self.send_sem, self.recv_sem = load_sem, send_sem, recv_sem
        self.keep, self.rows = master.shape[0] // n, master.shape[1]
        self.me = lax.axis_index("fs")

    def load(self, turn, peer):
        slot = lax.rem(turn, RING)
        return pltpu.make_async_copy(
            self.master.at[pl.ds(peer * self.keep, self.keep)], self.raw.at[slot], self.load_sem.at[slot]
        )

    def taken(self, turn):
        block = self.raw[lax.rem(turn, RING)]
        if self.gain is not None:
            block = block * self.gain[...][None]
        return block.astype(jnp.bfloat16)

    def cast(self, turn):
        self.send[turn] = self.taken(turn)

    def place(self, source):
        return self.held.at[:, span(source, self.rows), :]

    def keep_own(self, turn):
        self.held[:, span(self.me, self.rows), :] = self.taken(turn)

    def copy(self, turn, peer):
        return remote(
            self.send.at[turn], self.place(self.me), self.send_sem.at[peer], self.recv_sem.at[self.me], {"fs": peer}
        )

    def arrival(self, source):
        return remote(
            self.send.at[0], self.place(source), self.send_sem.at[source], self.recv_sem.at[source], {"fs": source}
        )


def kernel(
    n,
    tp,
    deep,
    gain,
    routes,
    affinity,
    prompt,
    gate,
    up,
    down,
    mixed_out,
    gate_out,
    up_out,
    down_out,
    raw_gate,
    raw_up,
    raw_down,
    send_gate,
    send_up,
    send_down,
    held_pair,
    held_down,
    prompt_in,
    token,
    info,
    gathered,
    passed,
    hidden,
    results,
    arrived,
    mixed,
    spread_weight,
    total,
    load_sem,
    weight_send,
    weight_recv,
    prompt_sem,
    token_send,
    token_recv,
    info_send,
    info_recv,
    pass_send,
    pass_recv,
    result_send,
    result_recv,
    part_send,
    part_recv,
    out_sem,
    *spreads,
):
    wide = n // deep
    keep, capacity = passed.shape[2], passed.shape[3]
    tokens, width = token.shape[1], token.shape[2]
    units = gate.shape[2]
    experts = keep * n
    me = lax.axis_index("fs")
    z, y = me // wide, lax.rem(me, wide)
    column = span(lax.axis_index("tp"), width)

    rows_spread = Spread(tp, gathered, capacity, width, spreads[:4])
    unit_spread = Spread(tp, hidden, wide * capacity, units, spreads[4:])
    pair = [
        Weights(
            n, master, gain, held_pair.at[:, :, i * units : (i + 1) * units], raw, send,
            load_sem.at[i], weight_send.at[i], weight_recv.at[i],
        )
        for i, (master, raw, send) in enumerate([(gate, raw_gate, send_gate), (up, raw_up, send_up)])
    ]
    lower = Weights(n, down, None, held_down, raw_down, send_down, load_sem.at[2], weight_send.at[2], weight_recv.at[2])

    def place(i):
        return far_first(z, deep, i)

    def peer(turn):
        return place(turn // wide) * wide + lax.rem(y + 1 + lax.rem(turn, wide), wide)

    barrier = pltpu.get_barrier_semaphore()
    for step in range(1, n):
        pl.semaphore_signal(barrier, inc=1, device_id={"fs": lax.rem(me + step, n)}, device_id_type=MESH)
    for hop in range(rows_spread.chips):
        pl.semaphore_signal(barrier, inc=1, device_id={"tp": rows_spread.target(hop)}, device_id_type=MESH)
    fetch = pltpu.make_async_copy(prompt, prompt_in, prompt_sem.at[0])
    fetch.start()
    for part in [*pair, lower]:
        for turn in range(RING):
            part.load(turn, peer(turn)).start()

    r0, r1 = routes[0:1, :], routes[1:2, :]
    names = lax.broadcasted_iota(jnp.int32, (experts, tokens), 0)
    hit0 = (names == r0).astype(jnp.float32)
    hit1 = (names == r1).astype(jnp.float32)
    before = lax.broadcasted_iota(jnp.int32, (tokens, tokens), 0)
    after = lax.broadcasted_iota(jnp.int32, (tokens, tokens), 1)
    earlier = jnp.where(before < after, 1.0, 0.0).astype(jnp.bfloat16)
    rank = jnp.dot((hit0 + hit1).astype(jnp.bfloat16), earlier, preferred_element_type=jnp.float32)
    a0, a1 = affinity[0:1, :], affinity[1:2, :]
    whole = a0 + a1
    info[z] = jnp.concatenate(
        [
            r0.astype(jnp.float32),
            r1.astype(jnp.float32),
            jnp.sum(hit0 * rank, axis=0, keepdims=True),
            jnp.sum(hit1 * rank, axis=0, keepdims=True),
            a0 / whole,
            a1 / whole,
            a0,
            a1,
        ],
        axis=0,
    )
    fetch.wait()
    tile = 128

    def normalize(i):
        rows = span(i, tile)
        values = prompt_in[rows, :].astype(jnp.float32)
        scale = lax.rsqrt(jnp.mean(values * values, axis=-1, keepdims=True) + norm_eps)
        token[z, rows, :] = (prompt_in[rows, column].astype(jnp.float32) * scale).astype(jnp.bfloat16)

    loop(0, tokens // tile, normalize)
    pl.semaphore_wait(barrier, n - 1 + rows_spread.chips)

    def onward(zs, side):
        where = {"fs": me + side * wide}
        return [
            remote(token.at[zs], token.at[zs], token_send.at[zs, (side + 1) // 2], token_recv.at[zs], where),
            remote(info.at[zs], info.at[zs], info_send.at[zs, (side + 1) // 2], info_recv.at[zs], where),
        ]

    def sends(zs, act):
        @pl.when((zs <= z) & (z < deep - 1))
        def _():
            for copy in onward(zs, 1):
                act(copy)

        @pl.when((zs >= z) & (z > 0))
        def _():
            for copy in onward(zs, -1):
                act(copy)

    def entry_slot(zs, expert):
        facts = info[zs]
        name = expert.astype(jnp.float32)
        first, second = facts[0:1, :] == name, facts[1:2, :] == name
        slot = jnp.where(first, facts[2:3, :], jnp.where(second, facts[3:4, :], -1.0))
        weight = jnp.where(first, facts[4:5, :], facts[5:6, :])
        return slot, weight

    slots = lax.broadcasted_iota(jnp.int32, (capacity, tokens), 0).astype(jnp.float32)

    def pick(zs, row, e):
        slot, _ = entry_slot(zs, (z * wide + row) * keep + e)
        chosen = jnp.where(slots == slot, 1.0, 0.0).astype(jnp.bfloat16)
        return jnp.dot(chosen, token[zs], preferred_element_type=jnp.float32).astype(jnp.bfloat16)

    def passing(zs, row):
        return remote(
            passed.at[zs, row],
            gathered.at[:, span(zs * wide + y, capacity), column],
            pass_send.at[zs, row],
            pass_recv.at[zs * wide + y],
            {"fs": z * wide + row},
        )

    def passing_in(zs, row):
        return remote(
            passed.at[zs, row],
            gathered.at[:, span(zs * wide + row, capacity), column],
            pass_send.at[zs, row],
            pass_recv.at[zs * wide + row],
            {"fs": z * wide + row},
        )

    def others(act):
        for step in range(1, wide):
            act(lax.rem(y + step, wide))

    def near_first(i):
        return place(deep - 1 - i)

    def extract(zs):
        def give(row):
            for e in range(keep):
                passed[zs, row, e] = pick(zs, row, e)
            passing(zs, row).start()

        others(give)
        for e in range(keep):
            gathered[e, span(zs * wide + y, capacity), column] = pick(zs, y, e)
        rows_spread.start(zs * wide + y)

    def take_passed(zs):
        def take(row):
            passing_in(zs, row).wait_recv()
            rows_spread.start(zs * wide + row)

        others(take)

    def hand_on_passed(zs):
        others(lambda row: rows_spread.hand_on(zs * wide + row))

    def give_weights(parts, first, last):
        def body(turn):
            target = peer(turn)
            for part in parts:
                part.load(turn, target).wait()
                part.cast(turn)

                @pl.when(turn + RING < n)
                def _():
                    part.load(turn + RING, peer(turn + RING)).start()

                part.copy(turn, target).start()

        loop(first, last, body)

    sends(z, lambda copy: copy.start())
    extract(z)

    def hop(i):
        zs = near_first(i)
        for copy in onward(zs, 0):
            copy.wait_recv()
        sends(zs, lambda copy: copy.start())
        extract(zs)
        before = near_first(i - 1)
        take_passed(before)
        rows_spread.hand_on(before * wide + y)

        @pl.when(i >= 2)
        def _():
            hand_on_passed(near_first(i - 2))

        first = jnp.where(i == 1, 0, (i - 1) * (n - 1) // deep)
        last = i * (n - 1) // deep
        give_weights(pair, first, last)

    loop(1, deep, hop)
    give_weights(pair, (deep - 1) * (n - 1) // deep, n - 1)
    final = near_first(deep - 1)
    take_passed(final)
    hand_on_passed(near_first(deep - 2))
    give_weights([lower], 0, n - 1)
    rows_spread.hand_on(final * wide + y)
    hand_on_passed(final)
    for part in [*pair, lower]:
        part.load(n - 1, me).wait()
        part.keep_own(n - 1)
    loop(0, n, rows_spread.arrive)

    def settle(zs):
        sends(zs, lambda copy: copy.wait_send())
        others(lambda row: passing(zs, row).wait_send())

    def all_in(parts):
        def body(step):
            source = lax.rem(me + step, n)
            for part in parts:
                part.arrival(source).wait_recv()

        loop(1, n, body)

    all_in(pair)
    keeping = [
        pltpu.make_async_copy(held_pair.at[:, :, :units], gate_out, out_sem.at[0]),
        pltpu.make_async_copy(held_pair.at[:, :, units:], up_out, out_sem.at[1]),
        pltpu.make_async_copy(held_down, down_out, out_sem.at[2]),
    ]
    keeping[0].start()
    keeping[1].start()
    unit_column = span(lax.axis_index("tp"), units)
    group = wide * capacity

    def produce(i):
        zs = place(i)
        for e in range(keep):
            both = jnp.dot(gathered[e, span(zs, group), :], held_pair[e], preferred_element_type=jnp.float32)
            gate_pre, up_pre = both[:, :units], both[:, units:]
            hidden[e, span(zs, group), unit_column] = (
                gate_pre / (1.0 + jnp.exp(-gate_pre)) * up_pre
            ).astype(jnp.bfloat16)
        unit_spread.start(zs)

    produce(0)

    def advance(i):
        produce(i)
        unit_spread.hand_on(place(i - 1))

    loop(1, deep, advance)
    unit_spread.hand_on(place(deep - 1))
    loop(0, deep, settle)
    loop(0, n, rows_spread.drain)
    all_in([lower])
    keeping[2].start()

    def returning(zs, row, mine):
        return remote(
            passed.at[zs, row],
            results.at[zs, mine],
            result_send.at[zs, row],
            result_recv.at[zs, mine],
            {"fs": z * wide + row},
        )

    def multiply(i):
        zs = place(i)
        unit_spread.arrive(zs)
        for e in range(keep):
            out = jnp.dot(
                hidden[e, span(zs, group), :], held_down[e], preferred_element_type=jnp.float32
            ).astype(jnp.bfloat16)
            for row in range(wide):
                part = out[row * capacity : (row + 1) * capacity]

                @pl.when(row == y)
                def _():
                    results[zs, row, e] = part

                @pl.when(row != y)
                def _():
                    passed[zs, row, e] = part

        others(lambda row: returning(zs, row, y).start())

    def add_up(zs):
        others(lambda row: returning(zs, row, row).wait_recv())
        for row in range(wide):
            for e in range(keep):
                slot, weight = entry_slot(zs, (z * wide + row) * keep + e)
                at = (row * keep + e) * capacity
                spread_weight[at : at + capacity, :] = jnp.where(slots == slot, weight, 0.0).astype(jnp.bfloat16)
        total[...] = lax.dot_general(
            spread_weight[...],
            results[zs].reshape(wide * keep * capacity, width),
            (((0,), (0,)), ((), ())),
            preferred_element_type=jnp.float32,
        )

    def part_copy(zs, side):
        last = zs == z + side
        at = jnp.where(last & (side < 0), deep, zs)
        return remote(token.at[zs], arrived.at[at], part_send.at[zs], part_recv.at[at], {"fs": me + side * wide})

    def part_in(at):
        return remote(token.at[0], arrived.at[at], part_send.at[0], part_recv.at[at], {"fs": me})

    def toward(zs):
        return jnp.where(zs > z, 1, -1)

    def send_part(i):
        zs = place(i)
        add_up(zs)
        fed = jnp.where(zs > z, z > 0, z < deep - 1)

        @pl.when(fed)
        def _():
            part_in(zs).wait_recv()
            token[zs] = (total[...] + arrived[zs].astype(jnp.float32)).astype(jnp.bfloat16)

        @pl.when(jnp.logical_not(fed))
        def _():
            token[zs] = total[...].astype(jnp.bfloat16)

        part_copy(zs, toward(zs)).start()

    multiply(0)

    def turn_back(i):
        multiply(i)
        send_part(i - 1)

    loop(1, deep, turn_back)
    add_up(z)

    @pl.when(z > 0)
    def _():
        part_in(z).wait_recv()
        total[...] += arrived[z].astype(jnp.float32)

    @pl.when(z < deep - 1)
    def _():
        part_in(deep).wait_recv()
        total[...] += arrived[deep].astype(jnp.float32)

    mixed[...] = total[...].astype(jnp.bfloat16)
    write = pltpu.make_async_copy(mixed, mixed_out, out_sem.at[3])
    write.start()

    def sent(turn):
        for part in [*pair, lower]:
            part.copy(turn, peer(turn)).wait_send()

    loop(0, n - 1, sent)
    loop(0, deep, unit_spread.drain)

    def sent_back(i):
        zs = place(i)
        others(lambda row: returning(zs, row, y).wait_send())

        @pl.when(zs != z)
        def _():
            part_copy(zs, toward(zs)).wait_send()

    loop(0, deep, sent_back)
    for copy in keeping:
        copy.wait()
    write.wait()


def per_device(prompt, routes, affinity, norm_gain, gate_master, up_master, down_master):
    n, tp = lax.axis_size("fs"), lax.axis_size("tp")
    chips = tp // 2
    deep = n // chips if n % chips == 0 else n
    wide = n // deep
    experts, rows, units = gate_master.shape
    _, unit_rows, width = down_master.shape
    tokens, model = prompt.shape
    keep = experts // n
    capacity = 2 * tokens * routes.shape[1] // experts
    inside, anywhere = pl.BlockSpec(memory_space=pltpu.VMEM), pl.BlockSpec(memory_space=pl.ANY)
    half, full = jnp.bfloat16, jnp.float32
    dma = pltpu.SemaphoreType.DMA
    mixed, gate_new, up_new, down_new = pl.pallas_call(
        functools.partial(kernel, n, tp, deep),
        out_shape=[
            jax.ShapeDtypeStruct((tokens, width), half),
            jax.ShapeDtypeStruct((keep, model, units), half),
            jax.ShapeDtypeStruct((keep, model, units), half),
            jax.ShapeDtypeStruct((keep, unit_rows * n, width), half),
        ],
        in_specs=[inside] * 3 + [anywhere] * 4,
        out_specs=[anywhere] * 4,
        scratch_shapes=[
            pltpu.VMEM((RING, keep, rows, units), full),
            pltpu.VMEM((RING, keep, rows, units), full),
            pltpu.VMEM((RING, keep, unit_rows, width), full),
            pltpu.VMEM((n - 1, keep, rows, units), half),
            pltpu.VMEM((n - 1, keep, rows, units), half),
            pltpu.VMEM((n - 1, keep, unit_rows, width), half),
            pltpu.VMEM((keep, model, 2 * units), half),
            pltpu.VMEM((keep, unit_rows * n, width), half),
            pltpu.VMEM((tokens, model), half),
            pltpu.VMEM((deep, tokens, width), half),
            pltpu.VMEM((deep, 8, tokens), full),
            pltpu.VMEM((keep, n * capacity, model), half),
            pltpu.VMEM((deep, wide, keep, capacity, width), half),
            pltpu.VMEM((keep, n * capacity, units * tp), half),
            pltpu.VMEM((deep, wide, keep, capacity, width), half),
            pltpu.VMEM((deep + 1, tokens, width), half),
            pltpu.VMEM((tokens, width), half),
            pltpu.VMEM((wide * keep * capacity, tokens), half),
            pltpu.VMEM((tokens, width), full),
            dma((3, RING)),
            dma((3, n)),
            dma((3, n)),
            dma((1,)),
            dma((deep, 2)),
            dma((deep,)),
            dma((deep, 2)),
            dma((deep,)),
            dma((deep, wide)),
            dma((n,)),
            dma((deep, wide)),
            dma((deep, wide)),
            dma((deep,)),
            dma((deep + 1,)),
            dma((4,)),
            *[dma((n, chips))] * 4,
            *[dma((deep, chips))] * 4,
        ],
        compiler_params=pltpu.CompilerParams(
            collective_id=0, has_side_effects=True, vmem_limit_bytes=63 * 2**20
        ),
        name="experts",
    )(norm_gain[:, None], routes.T, affinity.T, prompt, gate_master, up_master, down_master)
    return (mixed, gate_new, up_new, down_new)


def solution(mesh):
    in_specs = (
        P("fs", None),
        P("fs", None),
        P("fs", None),
        P("fs"),
        P(None, "fs", "tp"),
        P(None, "fs", "tp"),
        P(None, "fs", "tp"),
    )
    out_specs = (P("fs", "tp"), P("fs", None, "tp"), P("fs", None, "tp"), P("fs", None, "tp"))
    return jax.shard_map(
        per_device, mesh=mesh, in_specs=in_specs, out_specs=out_specs, check_vma=False
    )
```

```python
import functools

import jax
import jax.numpy as jnp
from jax import lax
from jax.experimental import pallas as pl
from jax.experimental.pallas import tpu as pltpu
from jax.sharding import PartitionSpec as P

norm_eps = 1e-06
MESH = pl.DeviceIdType.MESH
RING = 4
HALVES = 2


def remote(src, dst, send_sem, recv_sem, where):
    return pltpu.make_async_remote_copy(
        src_ref=src,
        dst_ref=dst,
        send_sem=send_sem,
        recv_sem=recv_sem,
        device_id=where,
        device_id_type=MESH,
    )


def loop(first, last, body):
    def step(i, carry):
        body(i)
        return carry

    lax.fori_loop(first, last, step, 0)


def span(index, size):
    return pl.ds(pl.multiple_of(index * size, size), size)


def far_first(z, depth, i):
    low, high = z, depth - 1 - z
    skew = jnp.abs(low - high)
    reach = jnp.minimum(low, high)
    j = i - skew
    distance = reach - j // 2
    paired = jnp.where((j % 2 == 0) == (low < high), z + distance, z - distance)
    single = jnp.where(low > high, i, depth - 1 - i)
    return jnp.where(i < skew, single, paired)


def giving_order(z, depth, i):
    left = z < depth - 1 - z
    outer = jnp.minimum(z, depth - 1 - z)
    own = 2 * outer + 1
    k = jnp.where(outer == 0, i - 1, i)
    j = jnp.where(k >= own, k + 1, k)
    inward = j // 2
    position = jnp.where((j % 2 == 0) == left, depth - 1 - inward, inward)
    beside = jnp.where(left, z + 1, z - 1)
    position = jnp.where((outer == 0) & (i == 0), beside, position)
    return jnp.where(i == depth - 1, z, position)


class Spread:
    def __init__(self, tp, whole, rows, width, sems):
        self.chips = tp // 2
        self.me = lax.axis_index("tp")
        self.chip, self.core = self.me // 2, self.me % 2
        self.whole, self.rows, self.width = whole, rows, width
        self.first_send, self.first_recv, self.relay_send, self.relay_recv = sems

    def target(self, hop):
        if hop == 0:
            return self.chip * 2 + 1 - self.core
        return lax.rem(self.chip + hop, self.chips) * 2 + self.core

    def block(self, chunk, owner):
        return self.whole.at[:, span(chunk, self.rows), span(owner, self.width)]

    def first(self, chunk, hop):
        mine = self.block(chunk, self.me)
        return remote(mine, mine, self.first_send.at[chunk, hop], self.first_recv.at[chunk, hop], {"tp": self.target(hop)})

    def relay(self, chunk, hop):
        owner = lax.rem(self.chip - hop + self.chips, self.chips) * 2 + self.core
        taken = self.block(chunk, owner)
        return remote(taken, taken, self.relay_send.at[chunk, hop], self.relay_recv.at[chunk, hop], {"tp": self.target(0)})

    def start(self, chunk):
        for hop in [*range(1, self.chips), 0]:
            self.first(chunk, hop).start()

    def hand_on(self, chunk):
        for hop in range(1, self.chips):
            self.first(chunk, hop).wait_recv()
            self.relay(chunk, hop).start()

    def arrive(self, chunk):
        self.first(chunk, 0).wait_recv()
        for hop in range(1, self.chips):
            self.relay(chunk, hop).wait_recv()

    def drain(self, chunk):
        for hop in range(self.chips):
            self.first(chunk, hop).wait_send()
        for hop in range(1, self.chips):
            self.relay(chunk, hop).wait_send()


def spread_sems(chunks, tp):
    return [pltpu.SemaphoreType.DMA((chunks, tp // 2))] * 4


class Weights:
    def __init__(self, n, master, gain, held, raw, send, load_sem, send_sem, recv_sem, cuts):
        self.n, self.master, self.gain, self.held, self.raw, self.send = n, master, gain, held, raw, send
        self.load_sem, self.send_sem, self.recv_sem = load_sem, send_sem, recv_sem
        self.keep, self.rows = master.shape[0] // n, master.shape[1]
        self.me = lax.axis_index("fs")
        size = master.shape[2] // cuts
        self.cuts = [slice(i * size, (i + 1) * size) for i in range(cuts)]

    def load(self, turn, peer):
        slot = lax.rem(turn, RING)
        return pltpu.make_async_copy(
            self.master.at[pl.ds(peer * self.keep, self.keep)], self.raw.at[slot], self.load_sem.at[slot]
        )

    def taken(self, turn):
        block = self.raw[lax.rem(turn, RING)]
        if self.gain is not None:
            block = block * self.gain[...][None]
        return block.astype(jnp.bfloat16)

    def cast(self, turn):
        self.send[turn] = self.taken(turn)

    def place(self, source):
        return self.held.at[:, span(source, self.rows), :]

    def keep_own(self, turn):
        self.held[:, span(self.me, self.rows), :] = self.taken(turn)

    def copies(self, turn, peer, cuts=(0, 1)):
        for cut in cuts[: len(self.cuts)]:
            part = self.cuts[cut]
            yield remote(
                self.send.at[turn, :, :, part],
                self.place(self.me).at[:, :, part],
                self.send_sem.at[peer, cut],
                self.recv_sem.at[self.me, cut],
                {"fs": peer},
            )

    def arrival(self, source, cut):
        part = self.cuts[cut]
        return remote(
            self.send.at[0, :, :, part],
            self.place(source).at[:, :, part],
            self.send_sem.at[source, cut],
            self.recv_sem.at[source, cut],
            {"fs": source},
        )


def kernel(
    n,
    tp,
    deep,
    gain,
    routes,
    affinity,
    prompt,
    gate,
    up,
    down,
    mixed_out,
    gate_out,
    up_out,
    down_out,
    raw_gate,
    raw_up,
    raw_down,
    send_gate,
    send_up,
    send_down,
    held_pair,
    held_down,
    prompt_in,
    token,
    info,
    gathered,
    passed,
    hidden,
    results,
    arrived,
    mixed,
    spread_weight,
    total,
    load_sem,
    weight_send,
    weight_recv,
    prompt_sem,
    token_send,
    token_recv,
    info_send,
    info_recv,
    pass_send,
    pass_recv,
    result_send,
    result_recv,
    part_send,
    part_recv,
    out_sem,
    *spreads,
):
    wide = n // deep
    keep, capacity = passed.shape[2], passed.shape[3]
    tokens, width = token.shape[1], token.shape[2]
    units = gate.shape[2]
    experts = keep * n
    me = lax.axis_index("fs")
    z, y = me // wide, lax.rem(me, wide)
    column = span(lax.axis_index("tp"), width)

    rows_spread = Spread(tp, gathered, capacity, width, spreads[:4])
    unit_spread = Spread(tp, hidden, wide * capacity, units, spreads[4:])
    pair = [
        Weights(
            n, master, gain, held_pair.at[:, :, i * units : (i + 1) * units], raw, send,
            load_sem.at[i], weight_send.at[i], weight_recv.at[i], 1,
        )
        for i, (master, raw, send) in enumerate([(gate, raw_gate, send_gate), (up, raw_up, send_up)])
    ]
    lower = Weights(
        n, down, None, held_down, raw_down, send_down, load_sem.at[2], weight_send.at[2], weight_recv.at[2], HALVES
    )

    def place(i):
        return far_first(z, deep, i)

    def peer(turn):
        return giving_order(z, deep, turn // wide) * wide + lax.rem(y + 1 + lax.rem(turn, wide), wide)

    barrier = pltpu.get_barrier_semaphore()
    for step in range(1, n):
        pl.semaphore_signal(barrier, inc=1, device_id={"fs": lax.rem(me + step, n)}, device_id_type=MESH)
    for hop in range(rows_spread.chips):
        pl.semaphore_signal(barrier, inc=1, device_id={"tp": rows_spread.target(hop)}, device_id_type=MESH)
    fetch = pltpu.make_async_copy(prompt, prompt_in, prompt_sem.at[0])
    fetch.start()
    for part in [*pair, lower]:
        for turn in range(RING):
            part.load(turn, peer(turn)).start()

    r0, r1 = routes[0:1, :], routes[1:2, :]
    names = lax.broadcasted_iota(jnp.int32, (experts, tokens), 0)
    hit0 = (names == r0).astype(jnp.float32)
    hit1 = (names == r1).astype(jnp.float32)
    before = lax.broadcasted_iota(jnp.int32, (tokens, tokens), 0)
    after = lax.broadcasted_iota(jnp.int32, (tokens, tokens), 1)
    earlier = jnp.where(before < after, 1.0, 0.0).astype(jnp.bfloat16)
    rank = jnp.dot((hit0 + hit1).astype(jnp.bfloat16), earlier, preferred_element_type=jnp.float32)
    a0, a1 = affinity[0:1, :], affinity[1:2, :]
    whole = a0 + a1
    info[z] = jnp.concatenate(
        [
            r0.astype(jnp.float32),
            r1.astype(jnp.float32),
            jnp.sum(hit0 * rank, axis=0, keepdims=True),
            jnp.sum(hit1 * rank, axis=0, keepdims=True),
            a0 / whole,
            a1 / whole,
            a0,
            a1,
        ],
        axis=0,
    )
    def give_weights(parts, first, last, cuts=(0, 1)):
        def body(turn):
            target = peer(turn)
            for part in parts:
                if 0 in cuts:
                    part.load(turn, target).wait()
                    part.cast(turn)

                    @pl.when(turn + RING < n)
                    def _():
                        part.load(turn + RING, peer(turn + RING)).start()

                for copy in part.copies(turn, target, cuts):
                    copy.start()

        loop(first, last, body)

    pl.semaphore_wait(barrier, n - 1 + rows_spread.chips)
    give_weights(pair[:1], 0, 1)
    fetch.wait()
    tile = 128

    def normalize(i):
        rows = span(i, tile)
        values = prompt_in[rows, :].astype(jnp.float32)
        scale = lax.rsqrt(jnp.mean(values * values, axis=-1, keepdims=True) + norm_eps)
        token[z, rows, :] = (prompt_in[rows, column].astype(jnp.float32) * scale).astype(jnp.bfloat16)

    loop(0, tokens // tile, normalize)

    def onward(zs, side):
        where = {"fs": me + side * wide}
        return [
            remote(token.at[zs], token.at[zs], token_send.at[zs, (side + 1) // 2], token_recv.at[zs], where),
            remote(info.at[zs], info.at[zs], info_send.at[zs, (side + 1) // 2], info_recv.at[zs], where),
        ]

    def sends(zs, act):
        @pl.when((zs <= z) & (z < deep - 1))
        def _():
            for copy in onward(zs, 1):
                act(copy)

        @pl.when((zs >= z) & (z > 0))
        def _():
            for copy in onward(zs, -1):
                act(copy)

    def entry_slot(zs, expert):
        facts = info[zs]
        name = expert.astype(jnp.float32)
        first, second = facts[0:1, :] == name, facts[1:2, :] == name
        slot = jnp.where(first, facts[2:3, :], jnp.where(second, facts[3:4, :], -1.0))
        weight = jnp.where(first, facts[4:5, :], facts[5:6, :])
        return slot, weight

    slots = lax.broadcasted_iota(jnp.int32, (capacity, tokens), 0).astype(jnp.float32)

    def pick(zs, row, e):
        slot, _ = entry_slot(zs, (z * wide + row) * keep + e)
        chosen = jnp.where(slots == slot, 1.0, 0.0).astype(jnp.bfloat16)
        return jnp.dot(chosen, token[zs], preferred_element_type=jnp.float32).astype(jnp.bfloat16)

    def passing(zs, row):
        return remote(
            passed.at[zs, row],
            gathered.at[:, span(zs * wide + y, capacity), column],
            pass_send.at[zs, row],
            pass_recv.at[zs * wide + y],
            {"fs": z * wide + row},
        )

    def passing_in(zs, row):
        return remote(
            passed.at[zs, row],
            gathered.at[:, span(zs * wide + row, capacity), column],
            pass_send.at[zs, row],
            pass_recv.at[zs * wide + row],
            {"fs": z * wide + row},
        )

    def others(act):
        for step in range(1, wide):
            act(lax.rem(y + step, wide))

    def near_first(i):
        return place(deep - 1 - i)

    def extract(zs):
        def give(row):
            for e in range(keep):
                passed[zs, row, e] = pick(zs, row, e)
            passing(zs, row).start()

        others(give)
        for e in range(keep):
            gathered[e, span(zs * wide + y, capacity), column] = pick(zs, y, e)
        rows_spread.start(zs * wide + y)

    def take_passed(zs):
        def take(row):
            passing_in(zs, row).wait_recv()
            rows_spread.start(zs * wide + row)

        others(take)

    def hand_on_passed(zs):
        others(lambda row: rows_spread.hand_on(zs * wide + row))

    end = (z == 0) | (z == deep - 1)
    to_line = (deep - 1) * wide

    def give_from_end():
        give_weights(pair[1:], 0, 1)
        give_weights(pair, 1, wide)
        give_weights([lower], 0, wide)
        give_weights(pair, wide, to_line)
        give_weights([lower], wide, to_line)

    def give_far():
        give_weights(pair[1:], 0, 1)
        give_weights(pair, 1, wide)

    def give_rest():
        give_weights(pair, wide, to_line)
        give_weights([lower], 0, 2 * wide)
        for cut in range(HALVES):
            give_weights([lower], 2 * wide, to_line, (cut,))

    sends(z, lambda copy: copy.start())
    extract(z)
    pl.when(end)(give_from_end)

    def hop(i):
        zs = near_first(i)
        for copy in onward(zs, 0):
            copy.wait_recv()
        sends(zs, lambda copy: copy.start())
        extract(zs)
        pl.when(jnp.logical_not(end) & (i == deep - 2))(give_far)
        pl.when(jnp.logical_not(end) & (i == deep - 1))(give_rest)
        before = near_first(i - 1)
        take_passed(before)
        rows_spread.hand_on(before * wide + y)

        @pl.when(i >= 2)
        def _():
            hand_on_passed(near_first(i - 2))

    loop(1, deep, hop)
    final = near_first(deep - 1)
    give_weights(pair, to_line, n - 1)
    give_weights([lower], to_line, n - 1)
    for part in [*pair, lower]:
        part.load(n - 1, me).wait()
        part.keep_own(n - 1)
    rows_spread.hand_on(final * wide + y)
    hand_on_passed(near_first(deep - 2))
    take_passed(final)
    hand_on_passed(final)
    loop(0, n, rows_spread.arrive)

    def settle(zs):
        sends(zs, lambda copy: copy.wait_send())
        others(lambda row: passing(zs, row).wait_send())

    def all_in(parts, cut):
        def body(step):
            source = lax.rem(me + step, n)
            for part in parts:
                part.arrival(source, cut).wait_recv()

        loop(1, n, body)

    all_in(pair, 0)
    keeping = [
        pltpu.make_async_copy(held_pair.at[:, :, :units], gate_out, out_sem.at[0]),
        pltpu.make_async_copy(held_pair.at[:, :, units:], up_out, out_sem.at[1]),
        pltpu.make_async_copy(held_down, down_out, out_sem.at[2]),
    ]
    keeping[0].start()
    keeping[1].start()
    unit_column = span(lax.axis_index("tp"), units)
    group = wide * capacity

    def produce(i):
        zs = place(i)
        for e in range(keep):
            both = jnp.dot(gathered[e, span(zs, group), :], held_pair[e], preferred_element_type=jnp.float32)
            gate_pre, up_pre = both[:, :units], both[:, units:]
            hidden[e, span(zs, group), unit_column] = (
                gate_pre / (1.0 + jnp.exp(-gate_pre)) * up_pre
            ).astype(jnp.bfloat16)
        unit_spread.start(zs)

    produce(0)

    def advance(i):
        produce(i)
        unit_spread.hand_on(place(i - 1))

    loop(1, deep, advance)
    unit_spread.hand_on(place(deep - 1))
    loop(0, deep, settle)
    loop(0, n, rows_spread.drain)

    half = width // HALVES

    def columns(cut):
        return slice(cut * half, (cut + 1) * half)

    def returning(zs, row, mine, cut):
        return remote(
            passed.at[zs, row, :, :, columns(cut)],
            results.at[zs, mine, :, :, columns(cut)],
            result_send.at[zs, row, cut],
            result_recv.at[zs, mine, cut],
            {"fs": z * wide + row},
        )

    def multiply(zs, cut):
        for e in range(keep):
            out = jnp.dot(
                hidden[e, span(zs, group), :], held_down[e, :, columns(cut)], preferred_element_type=jnp.float32
            ).astype(jnp.bfloat16)
            for row in range(wide):
                part = out[row * capacity : (row + 1) * capacity]

                @pl.when(row == y)
                def _():
                    results[zs, row, e, :, columns(cut)] = part

                @pl.when(row != y)
                def _():
                    passed[zs, row, e, :, columns(cut)] = part

        others(lambda row: returning(zs, row, y, cut).start())

    def add_up(zs, cut):
        others(lambda row: returning(zs, row, row, cut).wait_recv())
        for row in range(wide):
            for e in range(keep):
                slot, weight = entry_slot(zs, (z * wide + row) * keep + e)
                at = (row * keep + e) * capacity
                spread_weight[at : at + capacity, :] = jnp.where(slots == slot, weight, 0.0).astype(jnp.bfloat16)
        total[...] = lax.dot_general(
            spread_weight[...],
            results[zs, :, :, :, columns(cut)].reshape(wide * keep * capacity, half),
            (((0,), (0,)), ((), ())),
            preferred_element_type=jnp.float32,
        )

    def part_copy(zs, side, cut):
        last = zs == z + side
        at = jnp.where(last & (side < 0), deep, zs)
        return remote(
            token.at[zs, :, columns(cut)],
            arrived.at[at, :, columns(cut)],
            part_send.at[zs, cut],
            part_recv.at[at, cut],
            {"fs": me + side * wide},
        )

    def part_in(at, cut):
        return remote(
            token.at[0, :, columns(cut)],
            arrived.at[at, :, columns(cut)],
            part_send.at[0, cut],
            part_recv.at[at, cut],
            {"fs": me},
        )

    def toward(zs):
        return jnp.where(zs > z, 1, -1)

    def send_part(zs, cut):
        add_up(zs, cut)
        fed = jnp.where(zs > z, z > 0, z < deep - 1)

        @pl.when(fed)
        def _():
            part_in(zs, cut).wait_recv()
            token[zs, :, columns(cut)] = (
                total[...] + arrived[zs, :, columns(cut)].astype(jnp.float32)
            ).astype(jnp.bfloat16)

        @pl.when(jnp.logical_not(fed))
        def _():
            token[zs, :, columns(cut)] = total[...].astype(jnp.bfloat16)

        part_copy(zs, toward(zs), cut).start()

    def first_half(i):
        unit_spread.arrive(place(i))
        multiply(place(i), 0)

    all_in([lower], 0)
    first_half(0)

    def overlap(i):
        first_half(i)
        send_part(place(i - 1), 0)

    loop(1, deep - 1, overlap)
    first_half(deep - 1)
    for cut in range(1, HALVES):
        all_in([lower], cut)
        if cut == HALVES - 1:
            keeping[2].start()
        loop(0, deep, lambda i: multiply(place(i), cut))
        send_part(place(deep - 2), cut - 1)
        loop(0, deep - 2, lambda i: send_part(place(i), cut))
    send_part(place(deep - 2), HALVES - 1)
    writes = []
    for cut in range(HALVES):
        add_up(z, cut)

        @pl.when(z > 0)
        def _():
            part_in(z, cut).wait_recv()
            total[...] += arrived[z, :, columns(cut)].astype(jnp.float32)

        @pl.when(z < deep - 1)
        def _():
            part_in(deep, cut).wait_recv()
            total[...] += arrived[deep, :, columns(cut)].astype(jnp.float32)

        mixed[:, columns(cut)] = total[...].astype(jnp.bfloat16)
        write = pltpu.make_async_copy(
            mixed.at[:, columns(cut)], mixed_out.at[:, columns(cut)], out_sem.at[3 + cut]
        )
        write.start()
        writes.append(write)

    def sent(turn):
        for part in [*pair, lower]:
            for copy in part.copies(turn, peer(turn)):
                copy.wait_send()

    loop(0, n - 1, sent)
    loop(0, deep, unit_spread.drain)

    def sent_back(i):
        zs = place(i)
        for cut in range(HALVES):
            others(lambda row: returning(zs, row, y, cut).wait_send())

            @pl.when(zs != z)
            def _():
                part_copy(zs, toward(zs), cut).wait_send()

    loop(0, deep, sent_back)
    for copy in [*keeping, *writes]:
        copy.wait()


def per_device(prompt, routes, affinity, norm_gain, gate_master, up_master, down_master):
    n, tp = lax.axis_size("fs"), lax.axis_size("tp")
    chips = tp // 2
    deep = n // chips if n % chips == 0 else n
    wide = n // deep
    experts, rows, units = gate_master.shape
    _, unit_rows, width = down_master.shape
    tokens, model = prompt.shape
    keep = experts // n
    capacity = 2 * tokens * routes.shape[1] // experts
    inside, anywhere = pl.BlockSpec(memory_space=pltpu.VMEM), pl.BlockSpec(memory_space=pl.ANY)
    half, full = jnp.bfloat16, jnp.float32
    dma = pltpu.SemaphoreType.DMA
    mixed, gate_new, up_new, down_new = pl.pallas_call(
        functools.partial(kernel, n, tp, deep),
        out_shape=[
            jax.ShapeDtypeStruct((tokens, width), half),
            jax.ShapeDtypeStruct((keep, model, units), half),
            jax.ShapeDtypeStruct((keep, model, units), half),
            jax.ShapeDtypeStruct((keep, unit_rows * n, width), half),
        ],
        in_specs=[inside] * 3 + [anywhere] * 4,
        out_specs=[anywhere] * 4,
        scratch_shapes=[
            pltpu.VMEM((RING, keep, rows, units), full),
            pltpu.VMEM((RING, keep, rows, units), full),
            pltpu.VMEM((RING, keep, unit_rows, width), full),
            pltpu.VMEM((n - 1, keep, rows, units), half),
            pltpu.VMEM((n - 1, keep, rows, units), half),
            pltpu.VMEM((n - 1, keep, unit_rows, width), half),
            pltpu.VMEM((keep, model, 2 * units), half),
            pltpu.VMEM((keep, unit_rows * n, width), half),
            pltpu.VMEM((tokens, model), half),
            pltpu.VMEM((deep, tokens, width), half),
            pltpu.VMEM((deep, 8, tokens), full),
            pltpu.VMEM((keep, n * capacity, model), half),
            pltpu.VMEM((deep, wide, keep, capacity, width), half),
            pltpu.VMEM((keep, n * capacity, units * tp), half),
            pltpu.VMEM((deep, wide, keep, capacity, width), half),
            pltpu.VMEM((deep + 1, tokens, width), half),
            pltpu.VMEM((tokens, width), half),
            pltpu.VMEM((wide * keep * capacity, tokens), half),
            pltpu.VMEM((tokens, width // HALVES), full),
            dma((3, RING)),
            dma((3, n, HALVES)),
            dma((3, n, HALVES)),
            dma((1,)),
            dma((deep, 2)),
            dma((deep,)),
            dma((deep, 2)),
            dma((deep,)),
            dma((deep, wide)),
            dma((n,)),
            dma((deep, wide, HALVES)),
            dma((deep, wide, HALVES)),
            dma((deep, HALVES)),
            dma((deep + 1, HALVES)),
            dma((3 + HALVES,)),
            *[dma((n, chips))] * 4,
            *[dma((deep, chips))] * 4,
        ],
        compiler_params=pltpu.CompilerParams(
            collective_id=0, has_side_effects=True, vmem_limit_bytes=63 * 2**20
        ),
        name="experts",
    )(norm_gain[:, None], routes.T, affinity.T, prompt, gate_master, up_master, down_master)
    return (mixed, gate_new, up_new, down_new)


def solution(mesh):
    in_specs = (
        P("fs", None),
        P("fs", None),
        P("fs", None),
        P("fs"),
        P(None, "fs", "tp"),
        P(None, "fs", "tp"),
        P(None, "fs", "tp"),
    )
    out_specs = (P("fs", "tp"), P("fs", None, "tp"), P("fs", None, "tp"), P("fs", None, "tp"))
    return jax.shard_map(
        per_device, mesh=mesh, in_specs=in_specs, out_specs=out_specs, check_vma=False
    )
```

```python
import functools

import jax
import jax.numpy as jnp
from jax import lax
from jax.experimental import pallas as pl
from jax.experimental.pallas import tpu as pltpu
from jax.sharding import PartitionSpec as P

norm_eps = 1e-06
MESH = pl.DeviceIdType.MESH
RING = 4
HALVES = 2


def remote(src, dst, send_sem, recv_sem, where):
    return pltpu.make_async_remote_copy(
        src_ref=src,
        dst_ref=dst,
        send_sem=send_sem,
        recv_sem=recv_sem,
        device_id=where,
        device_id_type=MESH,
    )


def loop(first, last, body):
    def step(i, carry):
        body(i)
        return carry

    lax.fori_loop(first, last, step, 0)


def span(index, size):
    return pl.ds(pl.multiple_of(index * size, size), size)


def far_first(z, depth, i):
    low, high = z, depth - 1 - z
    skew = jnp.abs(low - high)
    reach = jnp.minimum(low, high)
    j = i - skew
    distance = reach - j // 2
    paired = jnp.where((j % 2 == 0) == (low < high), z + distance, z - distance)
    single = jnp.where(low > high, i, depth - 1 - i)
    return jnp.where(i < skew, single, paired)


def giving_order(z, depth, i):
    left = z < depth - 1 - z
    outer = jnp.minimum(z, depth - 1 - z)
    own = 2 * outer + 1
    j = jnp.where(i >= own, i + 1, i)
    inward = j // 2
    position = jnp.where((j % 2 == 0) == left, depth - 1 - inward, inward)
    outwards = jnp.where(left, i + 1, depth - 2 - i)
    position = jnp.where(outer == 0, outwards, position)
    return jnp.where(i == depth - 1, z, position)


class Spread:
    def __init__(self, tp, whole, rows, width, sems, groups=None):
        self.chips = tp // 2
        self.groups = groups
        self.me = lax.axis_index("tp")
        self.chip, self.core = self.me // 2, self.me % 2
        self.whole, self.rows, self.width = whole, rows, width
        self.first_send, self.first_recv, self.relay_send, self.relay_recv = sems

    def target(self, hop):
        if hop == 0:
            return self.chip * 2 + 1 - self.core
        return lax.rem(self.chip + hop, self.chips) * 2 + self.core

    def block(self, chunk, owner):
        if self.groups is None:
            return self.whole.at[:, span(chunk, self.rows), span(owner, self.width)]
        rows = span(lax.rem(chunk, self.groups), self.rows)
        return self.whole.at[chunk // self.groups, rows, span(owner, self.width)]

    def first(self, chunk, hop):
        mine = self.block(chunk, self.me)
        return remote(mine, mine, self.first_send.at[chunk, hop], self.first_recv.at[chunk, hop], {"tp": self.target(hop)})

    def relay(self, chunk, hop):
        owner = lax.rem(self.chip - hop + self.chips, self.chips) * 2 + self.core
        taken = self.block(chunk, owner)
        return remote(taken, taken, self.relay_send.at[chunk, hop], self.relay_recv.at[chunk, hop], {"tp": self.target(0)})

    def start(self, chunk):
        for hop in [*range(1, self.chips), 0]:
            self.first(chunk, hop).start()

    def hand_on(self, chunk):
        for hop in range(1, self.chips):
            self.first(chunk, hop).wait_recv()
            self.relay(chunk, hop).start()

    def arrive(self, chunk):
        self.first(chunk, 0).wait_recv()
        for hop in range(1, self.chips):
            self.relay(chunk, hop).wait_recv()

    def drain(self, chunk):
        for hop in range(self.chips):
            self.first(chunk, hop).wait_send()
        for hop in range(1, self.chips):
            self.relay(chunk, hop).wait_send()


def spread_sems(chunks, tp):
    return [pltpu.SemaphoreType.DMA((chunks, tp // 2))] * 4


class Weights:
    def __init__(self, n, master, gain, held, raw, send, load_sem, send_sem, recv_sem, cuts):
        self.n, self.master, self.gain, self.held, self.raw, self.send = n, master, gain, held, raw, send
        self.load_sem, self.send_sem, self.recv_sem = load_sem, send_sem, recv_sem
        self.keep, self.rows = master.shape[0] // n, master.shape[1]
        self.me = lax.axis_index("fs")
        if cuts is None:
            self.cuts = [(slice(e, e + 1), slice(None)) for e in range(self.keep)]
        else:
            size = master.shape[2] // cuts
            self.cuts = [(slice(None), slice(i * size, (i + 1) * size)) for i in range(cuts)]

    def load(self, turn, peer):
        slot = lax.rem(turn, RING)
        return pltpu.make_async_copy(
            self.master.at[pl.ds(peer * self.keep, self.keep)], self.raw.at[slot], self.load_sem.at[slot]
        )

    def taken(self, turn):
        block = self.raw[lax.rem(turn, RING)]
        if self.gain is not None:
            block = block * self.gain[...][None]
        return block.astype(jnp.bfloat16)

    def cast(self, turn):
        self.send[turn] = self.taken(turn)

    def place(self, source):
        return self.held.at[:, span(source, self.rows), :]

    def keep_own(self, turn):
        self.held[:, span(self.me, self.rows), :] = self.taken(turn)

    def copies(self, turn, peer, cuts=None):
        for cut in range(len(self.cuts)) if cuts is None else cuts:
            one, part = self.cuts[cut]
            yield remote(
                self.send.at[turn, one, :, part],
                self.place(self.me).at[one, :, part],
                self.send_sem.at[peer, cut],
                self.recv_sem.at[self.me, cut],
                {"fs": peer},
            )

    def arrival(self, source, cut):
        one, part = self.cuts[cut]
        return remote(
            self.send.at[0, one, :, part],
            self.place(source).at[one, :, part],
            self.send_sem.at[source, cut],
            self.recv_sem.at[source, cut],
            {"fs": source},
        )


def kernel(
    n,
    tp,
    deep,
    gain_row,
    routes,
    affinity,
    prompt,
    gate,
    up,
    down,
    mixed,
    held_pair,
    held_down,
    raw_gate,
    raw_up,
    raw_down,
    send_gate,
    send_up,
    send_down,
    prompt_in,
    token,
    info,
    gathered,
    passed,
    hidden,
    results,
    arrived,
    spread_weight,
    total,
    gain,
    load_sem,
    weight_send,
    weight_recv,
    prompt_sem,
    token_send,
    token_recv,
    info_send,
    info_recv,
    pass_send,
    pass_recv,
    result_send,
    result_recv,
    part_send,
    part_recv,
    *spreads,
):
    wide = n // deep
    keep, capacity = passed.shape[2], passed.shape[3]
    tokens, width = token.shape[1], token.shape[2]
    units = gate.shape[2]
    experts = keep * n
    me = lax.axis_index("fs")
    z, y = me // wide, lax.rem(me, wide)
    column = span(lax.axis_index("tp"), width)

    rows_spread = Spread(tp, gathered, capacity, width, spreads[:4])
    unit_spread = Spread(tp, hidden, wide * capacity, units, spreads[4:], deep)
    pair = [
        Weights(
            n, master, gain, held_pair.at[:, :, i * units : (i + 1) * units], raw, send,
            load_sem.at[i], weight_send.at[i], weight_recv.at[i], None,
        )
        for i, (master, raw, send) in enumerate([(gate, raw_gate, send_gate), (up, raw_up, send_up)])
    ]
    lower = Weights(
        n, down, None, held_down, raw_down, send_down, load_sem.at[2], weight_send.at[2], weight_recv.at[2], HALVES
    )

    def place(i):
        return far_first(z, deep, i)

    def peer(turn):
        return giving_order(z, deep, turn // wide) * wide + lax.rem(y + 1 + lax.rem(turn, wide), wide)

    barrier = pltpu.get_barrier_semaphore()
    for step in range(1, n):
        pl.semaphore_signal(barrier, inc=1, device_id={"fs": lax.rem(me + step, n)}, device_id_type=MESH)
    for hop in range(rows_spread.chips):
        pl.semaphore_signal(barrier, inc=1, device_id={"tp": rows_spread.target(hop)}, device_id_type=MESH)
    fetch = pltpu.make_async_copy(prompt, prompt_in, prompt_sem.at[0])
    fetch.start()
    for part in [*pair, lower]:
        for turn in range(RING):
            part.load(turn, peer(turn)).start()

    square = (gain.shape[0], gain.shape[0])
    diagonal = lax.broadcasted_iota(jnp.int32, square, 0) == lax.broadcasted_iota(jnp.int32, square, 1)
    gain[...] = jnp.sum(jnp.where(diagonal, gain_row[...], 0.0), axis=1, keepdims=True)

    r0, r1 = routes[0:1, :], routes[1:2, :]
    names = lax.broadcasted_iota(jnp.int32, (experts, tokens), 0)
    hit0 = (names == r0).astype(jnp.float32)
    hit1 = (names == r1).astype(jnp.float32)
    before = lax.broadcasted_iota(jnp.int32, (tokens, tokens), 0)
    after = lax.broadcasted_iota(jnp.int32, (tokens, tokens), 1)
    earlier = jnp.where(before < after, 1.0, 0.0).astype(jnp.bfloat16)
    rank = jnp.dot((hit0 + hit1).astype(jnp.bfloat16), earlier, preferred_element_type=jnp.float32)
    a0, a1 = affinity[0:1, :], affinity[1:2, :]
    whole = a0 + a1
    info[z] = jnp.concatenate(
        [
            r0.astype(jnp.float32),
            r1.astype(jnp.float32),
            jnp.sum(hit0 * rank, axis=0, keepdims=True),
            jnp.sum(hit1 * rank, axis=0, keepdims=True),
            a0 / whole,
            a1 / whole,
            a0,
            a1,
        ],
        axis=0,
    )
    def give_weights(parts, first, last, cuts=None):
        def body(turn):
            target = peer(turn)
            for part in parts:
                if cuts is None or 0 in cuts:
                    part.load(turn, target).wait()
                    part.cast(turn)

                    @pl.when(turn + RING < n)
                    def _():
                        part.load(turn + RING, peer(turn + RING)).start()

                for copy in part.copies(turn, target, cuts):
                    copy.start()

        loop(first, last, body)

    pl.semaphore_wait(barrier, n - 1 + rows_spread.chips)
    end = (z == 0) | (z == deep - 1)
    pl.when(jnp.logical_not(end))(lambda: give_weights(pair[:1], 0, 1, (0,)))
    fetch.wait()
    tile = 128

    def normalize(i):
        rows = span(i, tile)
        values = prompt_in[rows, :].astype(jnp.float32)
        scale = lax.rsqrt(jnp.mean(values * values, axis=-1, keepdims=True) + norm_eps)
        token[z, rows, :] = (prompt_in[rows, column].astype(jnp.float32) * scale).astype(jnp.bfloat16)

    loop(0, tokens // tile, normalize)

    def onward(zs, side):
        where = {"fs": me + side * wide}
        return [
            remote(token.at[zs], token.at[zs], token_send.at[zs, (side + 1) // 2], token_recv.at[zs], where),
            remote(info.at[zs], info.at[zs], info_send.at[zs, (side + 1) // 2], info_recv.at[zs], where),
        ]

    def sends(zs, act):
        @pl.when((zs <= z) & (z < deep - 1))
        def _():
            for copy in onward(zs, 1):
                act(copy)

        @pl.when((zs >= z) & (z > 0))
        def _():
            for copy in onward(zs, -1):
                act(copy)

    def entry_slot(zs, expert):
        facts = info[zs]
        name = expert.astype(jnp.float32)
        first, second = facts[0:1, :] == name, facts[1:2, :] == name
        slot = jnp.where(first, facts[2:3, :], jnp.where(second, facts[3:4, :], -1.0))
        weight = jnp.where(first, facts[4:5, :], facts[5:6, :])
        return slot, weight

    slots = lax.broadcasted_iota(jnp.int32, (capacity, tokens), 0).astype(jnp.float32)

    def pick(zs, row, e):
        slot, _ = entry_slot(zs, (z * wide + row) * keep + e)
        chosen = jnp.where(slots == slot, 1.0, 0.0).astype(jnp.bfloat16)
        return jnp.dot(chosen, token[zs], preferred_element_type=jnp.float32).astype(jnp.bfloat16)

    def passing(zs, row):
        return remote(
            passed.at[zs, row],
            gathered.at[:, span(zs * wide + y, capacity), column],
            pass_send.at[zs, row],
            pass_recv.at[zs * wide + y],
            {"fs": z * wide + row},
        )

    def passing_in(zs, row):
        return remote(
            passed.at[zs, row],
            gathered.at[:, span(zs * wide + row, capacity), column],
            pass_send.at[zs, row],
            pass_recv.at[zs * wide + row],
            {"fs": z * wide + row},
        )

    def others(act):
        for step in range(1, wide):
            act(lax.rem(y + step, wide))

    def near_first(i):
        return place(deep - 1 - i)

    def extract(zs):
        def give(row):
            for e in range(keep):
                passed[zs, row, e] = pick(zs, row, e)
            passing(zs, row).start()

        others(give)
        for e in range(keep):
            gathered[e, span(zs * wide + y, capacity), column] = pick(zs, y, e)
        rows_spread.start(zs * wide + y)

    def take_passed(zs):
        def take(row):
            passing_in(zs, row).wait_recv()
            rows_spread.start(zs * wide + row)

        others(take)

    def hand_on_passed(zs):
        others(lambda row: rows_spread.hand_on(zs * wide + row))

    to_line = (deep - 1) * wide

    rest = range(1, keep)

    def give_from_end():
        give_weights(pair, 0, wide)
        give_weights([lower], 0, 1)
        give_weights(pair, wide, to_line, (0,))
        give_weights(pair, wide, to_line, rest)
        give_weights([lower], 1, to_line)

    def give_far():
        give_weights(pair[1:], 0, 1, (0,))
        give_weights(pair, 1, wide, (0,))

    def give_rest():
        give_weights(pair, wide, 2 * wide)
        give_weights(pair, 2 * wide, to_line, (0,))
        give_weights(pair, 0, wide, rest)
        give_weights([lower], 0, wide, (0,))
        give_weights([lower], wide, 2 * wide)
        give_weights(pair, 2 * wide, to_line, rest)
        give_weights([lower], 2 * wide, to_line, (0,))
        for cut in range(1, HALVES):
            give_weights([lower], 0, wide, (cut,))
            give_weights([lower], 2 * wide, to_line, (cut,))

    sends(z, lambda copy: copy.start())
    extract(z)
    pl.when(end)(give_from_end)

    def hop(i):
        zs = near_first(i)
        for copy in onward(zs, 0):
            copy.wait_recv()
        sends(zs, lambda copy: copy.start())
        extract(zs)
        pl.when(jnp.logical_not(end) & (i == deep - 2))(give_far)
        pl.when(jnp.logical_not(end) & (i == deep - 1))(give_rest)
        before = near_first(i - 1)
        take_passed(before)
        rows_spread.hand_on(before * wide + y)

        @pl.when(i >= 2)
        def _():
            hand_on_passed(near_first(i - 2))

    loop(1, deep, hop)
    final = near_first(deep - 1)
    give_weights(pair, to_line, n - 1)
    give_weights([lower], to_line, n - 1)
    for part in [*pair, lower]:
        part.load(n - 1, me).wait()
        part.keep_own(n - 1)
    rows_spread.hand_on(final * wide + y)
    hand_on_passed(near_first(deep - 2))
    take_passed(final)
    hand_on_passed(final)
    loop(0, n, rows_spread.arrive)

    def settle(zs):
        sends(zs, lambda copy: copy.wait_send())
        others(lambda row: passing(zs, row).wait_send())

    def all_in(parts, cut):
        def body(step):
            source = lax.rem(me + step, n)
            for part in parts:
                part.arrival(source, cut).wait_recv()

        loop(1, n, body)

    unit_column = span(lax.axis_index("tp"), units)
    group = wide * capacity

    def produce(e):
        all_in(pair, e)

        def body(i):
            zs = place(i)
            both = jnp.dot(gathered[e, span(zs, group), :], held_pair[e], preferred_element_type=jnp.float32)
            gate_pre, up_pre = both[:, :units], both[:, units:]
            hidden[e, span(zs, group), unit_column] = (
                gate_pre / (1.0 + jnp.exp(-gate_pre)) * up_pre
            ).astype(jnp.bfloat16)
            unit_spread.start(e * deep + zs)

        loop(0, deep, body)

    for e in range(keep - 1):
        produce(e)
        loop(0, deep, lambda i: unit_spread.hand_on(e * deep + place(i)))
    loop(0, deep, settle)
    loop(0, n, rows_spread.drain)
    produce(keep - 1)

    half = width // HALVES

    def columns(cut):
        return slice(cut * half, (cut + 1) * half)

    def returning(zs, row, mine, cut):
        return remote(
            passed.at[zs, row, :, :, columns(cut)],
            results.at[zs, mine, :, :, columns(cut)],
            result_send.at[zs, row, cut],
            result_recv.at[zs, mine, cut],
            {"fs": z * wide + row},
        )

    def multiply(zs, cut):
        for e in range(keep):
            out = jnp.dot(
                hidden[e, span(zs, group), :], held_down[e, :, columns(cut)], preferred_element_type=jnp.float32
            ).astype(jnp.bfloat16)
            for row in range(wide):
                part = out[row * capacity : (row + 1) * capacity]

                @pl.when(row == y)
                def _():
                    results[zs, row, e, :, columns(cut)] = part

                @pl.when(row != y)
                def _():
                    passed[zs, row, e, :, columns(cut)] = part

        others(lambda row: returning(zs, row, y, cut).start())

    def add_up(zs, cut):
        others(lambda row: returning(zs, row, row, cut).wait_recv())
        for row in range(wide):
            for e in range(keep):
                slot, weight = entry_slot(zs, (z * wide + row) * keep + e)
                at = (row * keep + e) * capacity
                spread_weight[at : at + capacity, :] = jnp.where(slots == slot, weight, 0.0).astype(jnp.bfloat16)
        total[...] = lax.dot_general(
            spread_weight[...],
            results[zs, :, :, :, columns(cut)].reshape(wide * keep * capacity, half),
            (((0,), (0,)), ((), ())),
            preferred_element_type=jnp.float32,
        )

    def part_copy(zs, side, cut):
        last = zs == z + side
        at = jnp.where(last & (side < 0), deep, zs)
        return remote(
            token.at[zs, :, columns(cut)],
            arrived.at[at, :, columns(cut)],
            part_send.at[zs, cut],
            part_recv.at[at, cut],
            {"fs": me + side * wide},
        )

    def part_in(at, cut):
        return remote(
            token.at[0, :, columns(cut)],
            arrived.at[at, :, columns(cut)],
            part_send.at[0, cut],
            part_recv.at[at, cut],
            {"fs": me},
        )

    def toward(zs):
        return jnp.where(zs > z, 1, -1)

    def send_part(zs, cut):
        add_up(zs, cut)
        fed = jnp.where(zs > z, z > 0, z < deep - 1)

        @pl.when(fed)
        def _():
            part_in(zs, cut).wait_recv()
            token[zs, :, columns(cut)] = (
                total[...] + arrived[zs, :, columns(cut)].astype(jnp.float32)
            ).astype(jnp.bfloat16)

        @pl.when(jnp.logical_not(fed))
        def _():
            token[zs, :, columns(cut)] = total[...].astype(jnp.bfloat16)

        part_copy(zs, toward(zs), cut).start()

    def enter(i):
        unit_spread.hand_on((keep - 1) * deep + place(i))
        for e in range(keep):
            unit_spread.arrive(e * deep + place(i))

    enter(0)
    all_in([lower], 0)
    multiply(place(0), 0)

    def turn_back(i):
        enter(i + 1)
        multiply(place(i + 1), 0)

        @pl.when(i < deep - 2)
        def _():
            send_part(place(i), 0)

    loop(0, deep - 1, turn_back)
    for cut in range(1, HALVES):
        all_in([lower], cut)
        loop(0, deep, lambda i: multiply(place(i), cut))
        send_part(place(deep - 2), cut - 1)
        loop(0, deep - 2, lambda i: send_part(place(i), cut))
    send_part(place(deep - 2), HALVES - 1)
    for cut in range(HALVES):
        add_up(z, cut)

        @pl.when(z > 0)
        def _():
            part_in(z, cut).wait_recv()
            total[...] += arrived[z, :, columns(cut)].astype(jnp.float32)

        @pl.when(z < deep - 1)
        def _():
            part_in(deep, cut).wait_recv()
            total[...] += arrived[deep, :, columns(cut)].astype(jnp.float32)

        mixed[:, columns(cut)] = total[...].astype(jnp.bfloat16)

    def sent(turn):
        for part in [*pair, lower]:
            for copy in part.copies(turn, peer(turn)):
                copy.wait_send()

    loop(0, n - 1, sent)
    loop(0, keep * deep, unit_spread.drain)

    def sent_back(i):
        zs = place(i)
        for cut in range(HALVES):
            others(lambda row: returning(zs, row, y, cut).wait_send())

            @pl.when(zs != z)
            def _():
                part_copy(zs, toward(zs), cut).wait_send()

    loop(0, deep, sent_back)


def per_device(prompt, routes, affinity, norm_gain, gate_master, up_master, down_master):
    n, tp = lax.axis_size("fs"), lax.axis_size("tp")
    chips = tp // 2
    deep = n // chips if n % chips == 0 else n
    wide = n // deep
    experts, rows, units = gate_master.shape
    _, unit_rows, width = down_master.shape
    tokens, model = prompt.shape
    keep = experts // n
    capacity = 2 * tokens * routes.shape[1] // experts
    inside, anywhere = pl.BlockSpec(memory_space=pltpu.VMEM), pl.BlockSpec(memory_space=pl.ANY)
    half, full = jnp.bfloat16, jnp.float32
    dma = pltpu.SemaphoreType.DMA
    mixed, pair, down_new = pl.pallas_call(
        functools.partial(kernel, n, tp, deep),
        out_shape=[
            pltpu.VMEM((tokens, width), half),
            pltpu.VMEM((keep, model, 2 * units), half),
            pltpu.VMEM((keep, unit_rows * n, width), half),
        ],
        in_specs=[inside] * 3 + [anywhere] * 4,
        out_specs=[inside] * 3,
        scratch_shapes=[
            pltpu.VMEM((RING, keep, rows, units), full),
            pltpu.VMEM((RING, keep, rows, units), full),
            pltpu.VMEM((RING, keep, unit_rows, width), full),
            pltpu.VMEM((n - 1, keep, rows, units), half),
            pltpu.VMEM((n - 1, keep, rows, units), half),
            pltpu.VMEM((n - 1, keep, unit_rows, width), half),
            pltpu.VMEM((tokens, model), half),
            pltpu.VMEM((deep, tokens, width), half),
            pltpu.VMEM((deep, 8, tokens), full),
            pltpu.VMEM((keep, n * capacity, model), half),
            pltpu.VMEM((deep, wide, keep, capacity, width), half),
            pltpu.VMEM((keep, n * capacity, units * tp), half),
            pltpu.VMEM((deep, wide, keep, capacity, width), half),
            pltpu.VMEM((deep + 1, tokens, width), half),
            pltpu.VMEM((wide * keep * capacity, tokens), half),
            pltpu.VMEM((tokens, width // HALVES), full),
            pltpu.VMEM((rows, 1), full),
            dma((3, RING)),
            dma((3, n, HALVES)),
            dma((3, n, HALVES)),
            dma((1,)),
            dma((deep, 2)),
            dma((deep,)),
            dma((deep, 2)),
            dma((deep,)),
            dma((deep, wide)),
            dma((n,)),
            dma((deep, wide, HALVES)),
            dma((deep, wide, HALVES)),
            dma((deep, HALVES)),
            dma((deep + 1, HALVES)),
            *[dma((n, chips))] * 4,
            *[dma((keep * deep, chips))] * 4,
        ],
        compiler_params=pltpu.CompilerParams(
            collective_id=0, has_side_effects=True, vmem_limit_bytes=55 * 2**20
        ),
        name="experts",
    )(norm_gain[None, :], routes.T, affinity.T, prompt, gate_master, up_master, down_master)
    return (mixed, pair[:, :, :units], pair[:, :, units:], down_new)


def solution(mesh):
    in_specs = (
        P("fs", None),
        P("fs", None),
        P("fs", None),
        P("fs"),
        P(None, "fs", "tp"),
        P(None, "fs", "tp"),
        P(None, "fs", "tp"),
    )
    out_specs = (P("fs", "tp"), P("fs", None, "tp"), P("fs", None, "tp"), P("fs", None, "tp"))
    return jax.shard_map(
        per_device, mesh=mesh, in_specs=in_specs, out_specs=out_specs, check_vma=False
    )
```

```python
import functools

import jax
import jax.numpy as jnp
from jax import lax
from jax.experimental import pallas as pl
from jax.experimental.pallas import tpu as pltpu
from jax.sharding import PartitionSpec as P

norm_eps = 1e-06
MESH = pl.DeviceIdType.MESH
RING = 4
HALVES = 2


def remote(src, dst, send_sem, recv_sem, where):
    return pltpu.make_async_remote_copy(
        src_ref=src,
        dst_ref=dst,
        send_sem=send_sem,
        recv_sem=recv_sem,
        device_id=where,
        device_id_type=MESH,
    )


def loop(first, last, body):
    def step(i, carry):
        body(i)
        return carry

    lax.fori_loop(first, last, step, 0)


def span(index, size):
    return pl.ds(pl.multiple_of(index * size, size), size)


def far_first(z, depth, i):
    low, high = z, depth - 1 - z
    skew = jnp.abs(low - high)
    reach = jnp.minimum(low, high)
    j = i - skew
    distance = reach - j // 2
    paired = jnp.where((j % 2 == 0) == (low < high), z + distance, z - distance)
    single = jnp.where(low > high, i, depth - 1 - i)
    return jnp.where(i < skew, single, paired)


def giving_order(z, depth, i):
    left = z < depth - 1 - z
    outer = jnp.minimum(z, depth - 1 - z)
    own = 2 * outer + 1
    j = jnp.where(i >= own, i + 1, i)
    inward = j // 2
    position = jnp.where((j % 2 == 0) == left, depth - 1 - inward, inward)
    outwards = jnp.where(left, i + 1, depth - 2 - i)
    position = jnp.where(outer == 0, outwards, position)
    return jnp.where(i == depth - 1, z, position)


class Spread:
    def __init__(self, tp, whole, rows, width, sems, groups=None):
        self.chips = tp // 2
        self.groups = groups
        self.me = lax.axis_index("tp")
        self.chip, self.core = self.me // 2, self.me % 2
        self.whole, self.rows, self.width = whole, rows, width
        self.first_send, self.first_recv, self.relay_send, self.relay_recv = sems

    def target(self, hop):
        if hop == 0:
            return self.chip * 2 + 1 - self.core
        return lax.rem(self.chip + hop, self.chips) * 2 + self.core

    def block(self, chunk, owner):
        if self.groups is None:
            return self.whole.at[:, span(chunk, self.rows), span(owner, self.width)]
        rows = span(lax.rem(chunk, self.groups), self.rows)
        return self.whole.at[chunk // self.groups, rows, span(owner, self.width)]

    def first(self, chunk, hop):
        mine = self.block(chunk, self.me)
        return remote(mine, mine, self.first_send.at[chunk, hop], self.first_recv.at[chunk, hop], {"tp": self.target(hop)})

    def relay(self, chunk, hop):
        owner = lax.rem(self.chip - hop + self.chips, self.chips) * 2 + self.core
        taken = self.block(chunk, owner)
        return remote(taken, taken, self.relay_send.at[chunk, hop], self.relay_recv.at[chunk, hop], {"tp": self.target(0)})

    def start(self, chunk):
        for hop in [*range(1, self.chips), 0]:
            self.first(chunk, hop).start()

    def hand_on(self, chunk):
        for hop in range(1, self.chips):
            self.first(chunk, hop).wait_recv()
            self.relay(chunk, hop).start()

    def arrive(self, chunk):
        self.first(chunk, 0).wait_recv()
        for hop in range(1, self.chips):
            self.relay(chunk, hop).wait_recv()

    def drain(self, chunk):
        for hop in range(self.chips):
            self.first(chunk, hop).wait_send()
        for hop in range(1, self.chips):
            self.relay(chunk, hop).wait_send()


def spread_sems(chunks, tp):
    return [pltpu.SemaphoreType.DMA((chunks, tp // 2))] * 4


class Weights:
    def __init__(self, n, master, gain, held, raw, send, load_sem, send_sem, recv_sem, cuts):
        self.n, self.master, self.gain, self.held, self.raw, self.send = n, master, gain, held, raw, send
        self.load_sem, self.send_sem, self.recv_sem = load_sem, send_sem, recv_sem
        self.keep, self.rows = master.shape[0] // n, master.shape[1]
        self.me = lax.axis_index("fs")
        if cuts is None:
            self.cuts = [(slice(e, e + 1), slice(None)) for e in range(self.keep)]
        else:
            size = master.shape[2] // cuts
            self.cuts = [(slice(None), slice(i * size, (i + 1) * size)) for i in range(cuts)]

    def load(self, turn, peer):
        slot = lax.rem(turn, RING)
        return pltpu.make_async_copy(
            self.master.at[pl.ds(peer * self.keep, self.keep)], self.raw.at[slot], self.load_sem.at[slot]
        )

    def taken(self, turn):
        block = self.raw[lax.rem(turn, RING)]
        if self.gain is not None:
            block = block * self.gain[...][None]
        return block.astype(jnp.bfloat16)

    def cast(self, turn):
        self.send[turn] = self.taken(turn)

    def place(self, source):
        return self.held.at[:, span(source, self.rows), :]

    def keep_own(self, turn):
        self.held[:, span(self.me, self.rows), :] = self.taken(turn)

    def copies(self, turn, peer, cuts=None):
        for cut in range(len(self.cuts)) if cuts is None else cuts:
            one, part = self.cuts[cut]
            yield remote(
                self.send.at[turn, one, :, part],
                self.place(self.me).at[one, :, part],
                self.send_sem.at[peer, cut],
                self.recv_sem.at[self.me, cut],
                {"fs": peer},
            )

    def arrival(self, source, cut):
        one, part = self.cuts[cut]
        return remote(
            self.send.at[0, one, :, part],
            self.place(source).at[one, :, part],
            self.send_sem.at[source, cut],
            self.recv_sem.at[source, cut],
            {"fs": source},
        )


def kernel(
    n,
    tp,
    deep,
    gain_row,
    routes,
    affinity,
    prompt,
    gate,
    up,
    down,
    mixed,
    held_pair,
    held_down,
    raw_gate,
    raw_up,
    raw_down,
    send_gate,
    send_up,
    send_down,
    prompt_in,
    token,
    info,
    gathered,
    passed,
    hidden,
    results,
    arrived,
    spread_weight,
    total,
    own,
    gain,
    load_sem,
    weight_send,
    weight_recv,
    prompt_sem,
    token_send,
    token_recv,
    info_send,
    info_recv,
    pass_send,
    pass_recv,
    result_send,
    result_recv,
    part_send,
    part_recv,
    *spreads,
):
    wide = n // deep
    keep, capacity = passed.shape[2], passed.shape[3]
    tokens, width = token.shape[1], token.shape[2]
    units = gate.shape[2]
    experts = keep * n
    me = lax.axis_index("fs")
    z, y = me // wide, lax.rem(me, wide)
    column = span(lax.axis_index("tp"), width)

    rows_spread = Spread(tp, gathered, capacity, width, spreads[:4])
    unit_spread = Spread(tp, hidden, wide * capacity, units, spreads[4:], deep)
    pair = [
        Weights(
            n, master, gain, held_pair.at[:, :, i * units : (i + 1) * units], raw, send,
            load_sem.at[i], weight_send.at[i], weight_recv.at[i], None,
        )
        for i, (master, raw, send) in enumerate([(gate, raw_gate, send_gate), (up, raw_up, send_up)])
    ]
    lower = Weights(
        n, down, None, held_down, raw_down, send_down, load_sem.at[2], weight_send.at[2], weight_recv.at[2], HALVES
    )

    def place(i):
        return far_first(z, deep, i)

    def peer(turn):
        return giving_order(z, deep, turn // wide) * wide + lax.rem(y + 1 + lax.rem(turn, wide), wide)

    barrier = pltpu.get_barrier_semaphore()
    for step in range(1, n):
        pl.semaphore_signal(barrier, inc=1, device_id={"fs": lax.rem(me + step, n)}, device_id_type=MESH)
    for hop in range(rows_spread.chips):
        pl.semaphore_signal(barrier, inc=1, device_id={"tp": rows_spread.target(hop)}, device_id_type=MESH)
    fetch = pltpu.make_async_copy(prompt, prompt_in, prompt_sem.at[0])
    fetch.start()
    for part in [*pair, lower]:
        for turn in range(RING):
            part.load(turn, peer(turn)).start()

    square = (gain.shape[0], gain.shape[0])
    diagonal = lax.broadcasted_iota(jnp.int32, square, 0) == lax.broadcasted_iota(jnp.int32, square, 1)
    gain[...] = jnp.sum(jnp.where(diagonal, gain_row[...], 0.0), axis=1, keepdims=True)

    r0, r1 = routes[0:1, :], routes[1:2, :]
    names = lax.broadcasted_iota(jnp.int32, (experts, tokens), 0)
    hit0 = (names == r0).astype(jnp.float32)
    hit1 = (names == r1).astype(jnp.float32)
    before = lax.broadcasted_iota(jnp.int32, (tokens, tokens), 0)
    after = lax.broadcasted_iota(jnp.int32, (tokens, tokens), 1)
    earlier = jnp.where(before < after, 1.0, 0.0).astype(jnp.bfloat16)
    rank = jnp.dot((hit0 + hit1).astype(jnp.bfloat16), earlier, preferred_element_type=jnp.float32)
    a0, a1 = affinity[0:1, :], affinity[1:2, :]
    whole = a0 + a1
    info[z] = jnp.concatenate(
        [
            r0.astype(jnp.float32),
            r1.astype(jnp.float32),
            jnp.sum(hit0 * rank, axis=0, keepdims=True),
            jnp.sum(hit1 * rank, axis=0, keepdims=True),
            a0 / whole,
            a1 / whole,
            a0,
            a1,
        ],
        axis=0,
    )
    def give_weights(parts, first, last, cuts=None):
        def body(turn):
            target = peer(turn)
            for part in parts:
                if cuts is None or 0 in cuts:
                    part.load(turn, target).wait()
                    part.cast(turn)

                    @pl.when(turn + RING < n)
                    def _():
                        part.load(turn + RING, peer(turn + RING)).start()

                for copy in part.copies(turn, target, cuts):
                    copy.start()

        loop(first, last, body)

    pl.semaphore_wait(barrier, n - 1 + rows_spread.chips)
    end = (z == 0) | (z == deep - 1)
    pl.when(jnp.logical_not(end))(lambda: give_weights(pair[:1], 0, 1, (0,)))
    fetch.wait()
    tile = 128

    def normalize(i):
        rows = span(i, tile)
        values = prompt_in[rows, :].astype(jnp.float32)
        scale = lax.rsqrt(jnp.mean(values * values, axis=-1, keepdims=True) + norm_eps)
        token[z, rows, :] = (prompt_in[rows, column].astype(jnp.float32) * scale).astype(jnp.bfloat16)

    loop(0, tokens // tile, normalize)

    def onward(zs, side):
        where = {"fs": me + side * wide}
        return [
            remote(token.at[zs], token.at[zs], token_send.at[zs, (side + 1) // 2], token_recv.at[zs], where),
            remote(info.at[zs], info.at[zs], info_send.at[zs, (side + 1) // 2], info_recv.at[zs], where),
        ]

    def sends(zs, act):
        @pl.when((zs <= z) & (z < deep - 1))
        def _():
            for copy in onward(zs, 1):
                act(copy)

        @pl.when((zs >= z) & (z > 0))
        def _():
            for copy in onward(zs, -1):
                act(copy)

    def entry_slot(zs, expert):
        facts = info[zs]
        name = expert.astype(jnp.float32)
        first, second = facts[0:1, :] == name, facts[1:2, :] == name
        slot = jnp.where(first, facts[2:3, :], jnp.where(second, facts[3:4, :], -1.0))
        weight = jnp.where(first, facts[4:5, :], facts[5:6, :])
        return slot, weight

    slots = lax.broadcasted_iota(jnp.int32, (capacity, tokens), 0).astype(jnp.float32)

    def pick(zs, row, e):
        slot, _ = entry_slot(zs, (z * wide + row) * keep + e)
        chosen = jnp.where(slots == slot, 1.0, 0.0).astype(jnp.bfloat16)
        return jnp.dot(chosen, token[zs], preferred_element_type=jnp.float32).astype(jnp.bfloat16)

    def passing(zs, row):
        return remote(
            passed.at[zs, row],
            gathered.at[:, span(zs * wide + y, capacity), column],
            pass_send.at[zs, row],
            pass_recv.at[zs * wide + y],
            {"fs": z * wide + row},
        )

    def passing_in(zs, row):
        return remote(
            passed.at[zs, row],
            gathered.at[:, span(zs * wide + row, capacity), column],
            pass_send.at[zs, row],
            pass_recv.at[zs * wide + row],
            {"fs": z * wide + row},
        )

    def others(act):
        for step in range(1, wide):
            act(lax.rem(y + step, wide))

    def near_first(i):
        return place(deep - 1 - i)

    def extract(zs):
        def give(row):
            for e in range(keep):
                passed[zs, row, e] = pick(zs, row, e)
            passing(zs, row).start()

        others(give)
        for e in range(keep):
            gathered[e, span(zs * wide + y, capacity), column] = pick(zs, y, e)
        rows_spread.start(zs * wide + y)

    def take_passed(zs):
        def take(row):
            passing_in(zs, row).wait_recv()
            rows_spread.start(zs * wide + row)

        others(take)

    def hand_on_passed(zs):
        others(lambda row: rows_spread.hand_on(zs * wide + row))

    to_line = (deep - 1) * wide

    rest = range(1, keep)

    def give_from_end():
        give_weights(pair, 0, wide)
        give_weights([lower], 0, 1)
        give_weights(pair, wide, to_line, (0,))
        give_weights(pair, wide, to_line, rest)
        give_weights([lower], 1, to_line)

    def give_far():
        give_weights(pair[1:], 0, 1, (0,))
        give_weights(pair, 1, wide, (0,))

    def give_rest():
        give_weights(pair, wide, 2 * wide)
        give_weights(pair, 2 * wide, to_line, (0,))
        give_weights(pair, 0, wide, rest)
        give_weights([lower], 0, wide, (0,))
        give_weights([lower], wide, 2 * wide)
        give_weights(pair, 2 * wide, to_line, rest)
        give_weights([lower], 2 * wide, to_line, (0,))
        for cut in range(1, HALVES):
            give_weights([lower], 0, wide, (cut,))
            give_weights([lower], 2 * wide, to_line, (cut,))

    sends(z, lambda copy: copy.start())
    extract(z)
    pl.when(end)(give_from_end)

    def hop(i):
        zs = near_first(i)
        for copy in onward(zs, 0):
            copy.wait_recv()
        sends(zs, lambda copy: copy.start())
        extract(zs)
        pl.when(jnp.logical_not(end) & (i == deep - 2))(give_far)
        pl.when(jnp.logical_not(end) & (i == deep - 1))(give_rest)
        before = near_first(i - 1)
        take_passed(before)
        rows_spread.hand_on(before * wide + y)

        @pl.when(i >= 2)
        def _():
            hand_on_passed(near_first(i - 2))

    loop(1, deep, hop)
    final = near_first(deep - 1)
    give_weights(pair, to_line, n - 1)
    give_weights([lower], to_line, n - 1)
    for part in [*pair, lower]:
        part.load(n - 1, me).wait()
        part.keep_own(n - 1)
    rows_spread.hand_on(final * wide + y)
    hand_on_passed(near_first(deep - 2))
    take_passed(final)
    hand_on_passed(final)
    loop(0, n, rows_spread.arrive)

    def settle(zs):
        sends(zs, lambda copy: copy.wait_send())
        others(lambda row: passing(zs, row).wait_send())

    def all_in(parts, cut):
        def body(step):
            source = lax.rem(me + step, n)
            for part in parts:
                part.arrival(source, cut).wait_recv()

        loop(1, n, body)

    unit_column = span(lax.axis_index("tp"), units)
    group = wide * capacity

    def produce(e):
        all_in(pair, e)

        def body(i):
            zs = place(i)
            both = jnp.dot(gathered[e, span(zs, group), :], held_pair[e], preferred_element_type=jnp.float32)
            gate_pre, up_pre = both[:, :units], both[:, units:]
            hidden[e, span(zs, group), unit_column] = (
                gate_pre / (1.0 + jnp.exp(-gate_pre)) * up_pre
            ).astype(jnp.bfloat16)
            unit_spread.start(e * deep + zs)

        loop(0, deep, body)

    def weigh(zs):
        for row in range(wide):
            for e in range(keep):
                slot, weight = entry_slot(zs, (z * wide + row) * keep + e)
                at = (row * keep + e) * capacity
                spread_weight[zs, at : at + capacity, :] = jnp.where(slots == slot, weight, 0.0).astype(jnp.bfloat16)

    loop(0, deep, weigh)
    for e in range(keep - 1):
        produce(e)
        loop(0, deep, lambda i: unit_spread.hand_on(e * deep + place(i)))
    loop(0, deep, settle)
    loop(0, n, rows_spread.drain)
    produce(keep - 1)

    cuts = part_send.shape[1]
    per = cuts // HALVES
    half, piece = width // HALVES, width // cuts

    def columns(cut):
        return slice(cut * piece, (cut + 1) * piece)

    def returning(zs, row, mine, cut):
        return remote(
            passed.at[zs, row, :, :, columns(cut)],
            results.at[zs, mine, :, :, columns(cut)],
            result_send.at[zs, row, cut],
            result_recv.at[zs, mine, cut],
            {"fs": z * wide + row},
        )

    def multiply(zs, side):
        here = slice(side * half, (side + 1) * half)
        for e in range(keep):
            out = jnp.dot(
                hidden[e, span(zs, group), :], held_down[e, :, here], preferred_element_type=jnp.float32
            ).astype(jnp.bfloat16)
            for row in range(wide):
                part = out[row * capacity : (row + 1) * capacity]

                @pl.when(row == y)
                def _():
                    results[zs, row, e, :, here] = part

                @pl.when(row != y)
                def _():
                    passed[zs, row, e, :, here] = part

    def give_back(zs, cut):
        others(lambda row: returning(zs, row, y, cut).start())

    def summed(zs, cut):
        others(lambda row: returning(zs, row, row, cut).wait_recv())
        return lax.dot_general(
            spread_weight[zs],
            results[zs, :, :, :, columns(cut)].reshape(wide * keep * capacity, piece),
            (((0,), (0,)), ((), ())),
            preferred_element_type=jnp.float32,
        )

    def part_copy(zs, side, cut):
        last = zs == z + side
        at = jnp.where(last & (side < 0), deep, zs)
        return remote(
            token.at[zs, :, columns(cut)],
            arrived.at[at, :, columns(cut)],
            part_send.at[zs, cut],
            part_recv.at[at, cut],
            {"fs": me + side * wide},
        )

    def part_in(at, cut):
        return remote(
            token.at[0, :, columns(cut)],
            arrived.at[at, :, columns(cut)],
            part_send.at[0, cut],
            part_recv.at[at, cut],
            {"fs": me},
        )

    def toward(zs):
        return jnp.where(zs > z, 1, -1)

    def send_part(zs, cut):
        total[...] = summed(zs, cut)
        fed = jnp.where(zs > z, z > 0, z < deep - 1)

        @pl.when(fed)
        def _():
            part_in(zs, cut).wait_recv()
            token[zs, :, columns(cut)] = (
                total[...] + arrived[zs, :, columns(cut)].astype(jnp.float32)
            ).astype(jnp.bfloat16)

        @pl.when(jnp.logical_not(fed))
        def _():
            token[zs, :, columns(cut)] = total[...].astype(jnp.bfloat16)

        part_copy(zs, toward(zs), cut).start()

    def add_own(cut):
        own[:, columns(cut)] = summed(z, cut)

    def finish(cut):
        @pl.when(z > 0)
        def _():
            part_in(z, cut).wait_recv()
            own[:, columns(cut)] += arrived[z, :, columns(cut)].astype(jnp.float32)

        @pl.when(z < deep - 1)
        def _():
            part_in(deep, cut).wait_recv()
            own[:, columns(cut)] += arrived[deep, :, columns(cut)].astype(jnp.float32)

        mixed[:, columns(cut)] = own[:, columns(cut)].astype(jnp.bfloat16)

    def enter(i):
        unit_spread.hand_on((keep - 1) * deep + place(i))
        for e in range(keep):
            unit_spread.arrive(e * deep + place(i))

    def give_back_all(zs, first, last):
        for cut in range(first, last):
            give_back(zs, cut)

    def send_all(zs, first, last):
        for cut in range(first, last):
            send_part(zs, cut)

    def come(i):
        enter(i)
        multiply(place(i), 0)
        give_back_all(place(i), 0, per)

    lead = deep - 2
    inner = jnp.logical_not(end)
    enter(0)
    all_in([lower], 0)
    multiply(place(0), 0)
    give_back_all(place(0), 0, per)

    def second(i):
        multiply(place(i), 1)
        give_back_all(place(i), per, cuts)

    def lead_in(i):
        come(i)

        @pl.when(inner & (i == 1))
        def _():
            all_in([lower], 1)
            second(0)

        send_all(place(i - 1), 0, per)

    loop(1, lead, lead_in)
    pl.when(inner)(lambda: loop(1, lead, second))
    send_all(place(lead - 1), 0, per)
    loop(lead, deep, come)

    @pl.when(end)
    def _():
        all_in([lower], 1)
        loop(0, lead, second)

    pl.when(end)(lambda: send_part(place(lead), 0))
    loop(lead, deep, second)

    def lead_out(i):
        send_all(place(i), per, cuts)

        @pl.when(inner & (i == 0))
        def _():
            send_all(place(lead), 0, per)

    loop(0, lead, lead_out)

    @pl.when(end)
    def _():
        send_all(place(lead), 1, per)

    send_all(place(lead), per, cuts)
    for cut in range(cuts):
        add_own(cut)

    def sent(turn):
        for part in [*pair, lower]:
            for copy in part.copies(turn, peer(turn)):
                copy.wait_send()

    loop(0, n - 1, sent)
    loop(0, keep * deep, unit_spread.drain)
    for cut in range(cuts):
        finish(cut)

    def sent_back(i):
        zs = place(i)
        for cut in range(cuts):
            others(lambda row: returning(zs, row, y, cut).wait_send())

            @pl.when(zs != z)
            def _():
                part_copy(zs, toward(zs), cut).wait_send()

    loop(0, deep, sent_back)


def per_device(prompt, routes, affinity, norm_gain, gate_master, up_master, down_master):
    n, tp = lax.axis_size("fs"), lax.axis_size("tp")
    chips = tp // 2
    deep = n // chips if n % chips == 0 else n
    wide = n // deep
    experts, rows, units = gate_master.shape
    _, unit_rows, width = down_master.shape
    tokens, model = prompt.shape
    keep = experts // n
    cuts = 2 * HALVES if width % (2 * HALVES * 128) == 0 else HALVES
    capacity = 2 * tokens * routes.shape[1] // experts
    inside, anywhere = pl.BlockSpec(memory_space=pltpu.VMEM), pl.BlockSpec(memory_space=pl.ANY)
    half, full = jnp.bfloat16, jnp.float32
    dma = pltpu.SemaphoreType.DMA
    mixed, pair, down_new = pl.pallas_call(
        functools.partial(kernel, n, tp, deep),
        out_shape=[
            pltpu.VMEM((tokens, width), half),
            pltpu.VMEM((keep, model, 2 * units), half),
            pltpu.VMEM((keep, unit_rows * n, width), half),
        ],
        in_specs=[inside] * 3 + [anywhere] * 4,
        out_specs=[inside] * 3,
        scratch_shapes=[
            pltpu.VMEM((RING, keep, rows, units), full),
            pltpu.VMEM((RING, keep, rows, units), full),
            pltpu.VMEM((RING, keep, unit_rows, width), full),
            pltpu.VMEM((n - 1, keep, rows, units), half),
            pltpu.VMEM((n - 1, keep, rows, units), half),
            pltpu.VMEM((n - 1, keep, unit_rows, width), half),
            pltpu.VMEM((tokens, model), half),
            pltpu.VMEM((deep, tokens, width), half),
            pltpu.VMEM((deep, 8, tokens), full),
            pltpu.VMEM((keep, n * capacity, model), half),
            pltpu.VMEM((deep, wide, keep, capacity, width), half),
            pltpu.VMEM((keep, n * capacity, units * tp), half),
            pltpu.VMEM((deep, wide, keep, capacity, width), half),
            pltpu.VMEM((deep + 1, tokens, width), half),
            pltpu.VMEM((deep, wide * keep * capacity, tokens), half),
            pltpu.VMEM((tokens, width // cuts), full),
            pltpu.VMEM((tokens, width), full),
            pltpu.VMEM((rows, 1), full),
            dma((3, RING)),
            dma((3, n, HALVES)),
            dma((3, n, HALVES)),
            dma((1,)),
            dma((deep, 2)),
            dma((deep,)),
            dma((deep, 2)),
            dma((deep,)),
            dma((deep, wide)),
            dma((n,)),
            dma((deep, wide, cuts)),
            dma((deep, wide, cuts)),
            dma((deep, cuts)),
            dma((deep + 1, cuts)),
            *[dma((n, chips))] * 4,
            *[dma((keep * deep, chips))] * 4,
        ],
        compiler_params=pltpu.CompilerParams(
            collective_id=0, has_side_effects=True, vmem_limit_bytes=56 * 2**20
        ),
        name="experts",
    )(norm_gain[None, :], routes.T, affinity.T, prompt, gate_master, up_master, down_master)
    return (mixed, pair[:, :, :units], pair[:, :, units:], down_new)


def solution(mesh):
    in_specs = (
        P("fs", None),
        P("fs", None),
        P("fs", None),
        P("fs"),
        P(None, "fs", "tp"),
        P(None, "fs", "tp"),
        P(None, "fs", "tp"),
    )
    out_specs = (P("fs", "tp"), P("fs", None, "tp"), P("fs", None, "tp"), P("fs", None, "tp"))
    return jax.shard_map(
        per_device, mesh=mesh, in_specs=in_specs, out_specs=out_specs, check_vma=False
    )
```
